256 devices in a mesh: sp: 32 (over z, y), tp: 8 (over x, core).
Axes of the slice: x: 4, y: 4, z: 8, core: 2. Of those that a mesh axis runs over, the one named last changes fastest.
Arguments:
- inputs: bfloat16 [16384, 2048], P('sp', 'tp'), may hold values from -6 to 6
- norm_gain: float32 [2048], replicated, may hold values from 0.1 to 1.9
- latent_query: bfloat16 [2048, 1536], P(None, 'tp'), may hold values from -2 to 2
- latent_down: bfloat16 [2048, 512], replicated, may hold values from -2 to 2
- rope_down: bfloat16 [2048, 32], replicated, may hold values from -2 to 2
- latent_gain: float32 [512], replicated, may hold values from 0.1 to 1.9
- latent_up: bfloat16 [512, 2048], P(None, 'tp'), may hold values from -2 to 2
- window_query: bfloat16 [2048, 1024], P(None, 'tp'), may hold values from -2 to 2
- window_key: bfloat16 [2048, 512], P(None, 'tp'), may hold values from -2 to 2
- window_value: bfloat16 [2048, 512], P(None, 'tp'), may hold values from -0.125 to 0.125
- sink_logit: float32 [16], P('tp'), may hold values from 3 to 8
- out_latent: bfloat16 [1024, 2048], P('tp'), may hold values from -0.1875 to 0.1875
- out_window: bfloat16 [1024, 2048], P('tp'), may hold values from -0.1875 to 0.1875
Outputs:
- attended: bfloat16 [16384, 2048], P('sp', 'tp')
The draws below stay inside these ranges and needn't reach their ends.
All inputs are finite; a program needn't handle non-finite values.
Results may differ from the reference program's by a relative error of at most 0.017.
Values may be sent and summed in bfloat16 or wider, within the bound.
A program may use at most 128 MiB of HBM per device.

```python
import jax
import jax.numpy as jnp
from jax import lax

D = 2048
HM = 16
HS = 16
HK = 8
LATENT = 512
NOPE = 64
ROPE = 32
HEAD = 64
WINDOW = 128
TOKENS = 16384
N_TP = 8


def latent_tables(key):
    streams = jax.random.split(jax.random.fold_in(key, 7001), 5)
    lowering = jax.random.normal(streams[0], (D, LATENT), jnp.float32) * D ** (-0.5)
    rotating = jax.random.normal(streams[1], (D, ROPE), jnp.float32) * D ** (-0.5)
    raising = jax.random.normal(streams[2], (LATENT, HM * (NOPE + HEAD)), jnp.float32) * LATENT ** (-0.5)
    queries = jax.random.normal(streams[4], (D, HM * (NOPE + ROPE)), jnp.float32) * 2.5 * D ** (-0.5)
    return (jnp.clip(queries, -2.0, 2.0), jnp.clip(lowering, -2.0, 2.0), jnp.clip(rotating, -2.0, 2.0), jnp.clip(raising, -2.0, 2.0))


def window_tables(key):
    streams = jax.random.split(jax.random.fold_in(key, 7002), 3)
    key_weights = jax.random.normal(streams[0], (D, HK * HEAD), jnp.float32) * D ** (-0.5)
    queries = jax.random.normal(streams[2], (D, HS * HEAD), jnp.float32) * 2.0 * D ** (-0.5)
    return (jnp.clip(queries, -2.0, 2.0), jnp.clip(key_weights, -2.0, 2.0))


def draw_latent_query(key, part):
    return latent_tables(key)[0].astype(jnp.bfloat16)


def draw_latent_down(key, part):
    return latent_tables(key)[1].astype(jnp.bfloat16)


def draw_rope_down(key, part):
    return latent_tables(key)[2].astype(jnp.bfloat16)


def draw_latent_up(key, part):
    return latent_tables(key)[3].astype(jnp.bfloat16)


def draw_window_query(key, part):
    return window_tables(key)[0].astype(jnp.bfloat16)


def draw_window_key(key, part):
    return window_tables(key)[1].astype(jnp.bfloat16)


def level_of(key, dims, pieces, smallest, top_value):
    def one(dim, blocks):
        steps = jax.random.uniform(jax.random.fold_in(jax.random.fold_in(key, 6), dim), (blocks,), jnp.float32, smallest / len(pieces), top_value / len(pieces))
        return jnp.repeat(jnp.exp(steps), dims[dim] // blocks).reshape((-1,) + (1,) * (len(dims) - dim - 1))

    level = one(*pieces[0])
    for cut in pieces[1:]:
        level = level * one(*cut)
    return level


def centred(stream_key, dims, width, most, cuts=(), kind=jnp.bfloat16):
    values = jax.random.normal(stream_key, dims, jnp.float32) * width
    if len(cuts) > 0:
        values = level_of(stream_key, dims, cuts, -0.22, 0.18) * values
    return jnp.clip(values, min=-most, max=most).astype(kind)


def setup_inputs(seed: int = 0) -> dict:
    splits = jax.random.split(jax.random.key(seed), 14)
    return {
        "inputs": centred(splits[0], (TOKENS, D), 1.0, 6.0, ((0, 32), (1, 8))),
        "norm_gain": jnp.clip(1.0 + 0.18 * jax.random.normal(splits[1], (D,), jnp.float32), 0.1, 1.9),
        "latent_query": draw_latent_query(jax.random.fold_in(splits[13], 71), 0),
        "latent_down": draw_latent_down(jax.random.fold_in(splits[13], 71), 0),
        "rope_down": draw_rope_down(jax.random.fold_in(splits[13], 71), 0),
        "latent_gain": jnp.clip(1.0 + 0.18 * jax.random.normal(splits[5], (LATENT,), jnp.float32), 0.1, 1.9),
        "latent_up": draw_latent_up(jax.random.fold_in(splits[13], 71), 0),
        "window_query": draw_window_query(jax.random.fold_in(splits[13], 71), 0),
        "window_key": draw_window_key(jax.random.fold_in(splits[13], 71), 0),
        "window_value": centred(splits[9], (D, HK * HEAD), D ** -0.5, 0.125, ((1, 8),)),
        "sink_logit": jnp.clip(3.0 + 5.0 * jax.random.uniform(splits[10], (HS,), jnp.float32) ** level_of(splits[10], (HS,), ((0, 8),), -0.2, 0.2), 3.0, 8.0),
        "out_latent": centred(splits[11], (HM * HEAD, D), (HM * HEAD) ** -0.5, 0.1875, ((0, 8),)),
        "out_window": centred(splits[12], (HS * HEAD, D), (HS * HEAD) ** -0.5, 0.1875, ((0, 8),)),
    }


epsilon = 1e-06

def rms_scale(values, gains):
    return values * lax.rsqrt(lax.optimization_barrier(jnp.mean(values * values, axis=-1, keepdims=True)) + epsilon) * gains

def rotary(values, positions):
    half_width = values.shape[-1] // 2
    inverse = 1.0 / 10000.0 ** (jnp.arange(0, 2 * half_width, 2).astype(jnp.float32) / (2 * half_width))
    angles = positions[:, None] * inverse[None, :]
    cosine_table = jnp.cos(angles)[:, None, :]
    sine_table = jnp.sin(angles)[:, None, :]
    first_half = values[..., :half_width]
    second_half = values[..., half_width:]
    return jnp.concatenate([first_half * cosine_table - second_half * sine_table, second_half * cosine_table + first_half * sine_table], axis=-1)

def reference(inputs, norm_gain, latent_query, latent_down, rope_down, latent_gain, latent_up, window_query, window_key, window_value, sink_logit, out_latent, out_window):
    length_all = inputs.shape[0]
    positions = jnp.arange(length_all).astype(jnp.float32)
    hidden = rms_scale(inputs.astype(jnp.float32), norm_gain).astype(jnp.bfloat16)
    latent = rms_scale(jnp.dot(hidden, latent_down, preferred_element_type=jnp.float32), latent_gain).astype(jnp.bfloat16)
    shared = rotary(jnp.dot(hidden, rope_down, preferred_element_type=jnp.float32)[:, None, :], positions)[:, 0, :].astype(jnp.bfloat16)
    expanded = jnp.dot(latent, latent_up, preferred_element_type=jnp.float32).astype(jnp.bfloat16)
    expanded = expanded.reshape(length_all, HM, NOPE + HEAD)
    queries = jnp.dot(hidden, latent_query, preferred_element_type=jnp.float32).reshape(length_all, HM, NOPE + ROPE)
    queries = jnp.concatenate([queries[..., :NOPE], rotary(queries[..., NOPE:], positions)], axis=-1).astype(jnp.bfloat16)
    key_plain = expanded[..., :NOPE].astype(jnp.float32)
    value_rows = expanded[..., NOPE:].astype(jnp.float32)
    shared_rows = shared.astype(jnp.float32)
    score_scale = (NOPE + ROPE) ** (-0.5)

    def latent_block(query_block):
        query_block = query_block.astype(jnp.float32)
        scores = (jnp.einsum('qhn,khn->hqk', query_block[..., :NOPE], key_plain) + jnp.einsum('qhr,kr->hqk', query_block[..., NOPE:], shared_rows)) * score_scale
        highest = lax.optimization_barrier(jnp.max(scores, axis=-1, keepdims=True))
        weights = jnp.exp(scores - highest)
        summed = lax.optimization_barrier(jnp.sum(weights, axis=-1))
        rounded = lax.optimization_barrier(weights.astype(jnp.bfloat16)).astype(jnp.float32)
        mixture = jnp.einsum('hqk,khd->qhd', rounded, value_rows)
        return mixture / jnp.transpose(summed)[:, :, None]
    query_blocks = queries.reshape(length_all // WINDOW, WINDOW, HM, NOPE + ROPE)
    latent_out = lax.map(latent_block, query_blocks).reshape(length_all, HM * HEAD).astype(jnp.bfloat16)
    group_size = HS // HK
    block_count = length_all // WINDOW
    window_queries = rotary(jnp.dot(hidden, window_query, preferred_element_type=jnp.float32).reshape(length_all, HS, HEAD), positions).astype(jnp.bfloat16)
    window_keys = rotary(jnp.dot(hidden, window_key, preferred_element_type=jnp.float32).reshape(length_all, HK, HEAD), positions).astype(jnp.bfloat16)
    window_values = jnp.dot(hidden, window_value, preferred_element_type=jnp.float32).astype(jnp.bfloat16).reshape(length_all, HK, HEAD)

    def banded(values):
        padded = jnp.pad(values, ((WINDOW, WINDOW), (0, 0), (0, 0)))
        grid_rows = padded.reshape(block_count + 2, WINDOW, HK, HEAD)
        return jnp.concatenate([grid_rows[:-2], grid_rows[1:-1], grid_rows[2:]], axis=1)
    band_keys = banded(window_keys).astype(jnp.float32)
    band_values = banded(window_values).astype(jnp.float32)
    query_band = window_queries.reshape(block_count, WINDOW, HK, group_size, HEAD).astype(jnp.float32)
    offsets = jnp.arange(3 * WINDOW)[None, :] - jnp.arange(WINDOW)[:, None]
    key_pos = jnp.arange(block_count)[:, None] * WINDOW - WINDOW + jnp.arange(3 * WINDOW)[None, :]
    allowed = ((offsets >= 0) & (offsets <= 2 * WINDOW))[None] & ((key_pos >= 0) & (key_pos < length_all))[:, None, :]
    sink_table = sink_logit.reshape(HK, group_size)

    def window_head(operands):
        head_queries, head_keys, head_values, head_sinks = operands
        scores = jnp.einsum('nqgd,nkd->ngqk', head_queries, head_keys) * HEAD ** (-0.5)
        scores = jnp.where(allowed[:, None], scores, -jnp.inf)
        highest = jnp.maximum(lax.optimization_barrier(jnp.max(scores, axis=-1)), head_sinks[None, :, None])
        weights = jnp.exp(scores - highest[..., None])
        summed = lax.optimization_barrier(jnp.sum(weights, axis=-1)) + jnp.exp(head_sinks[None, :, None] - highest)
        rounded = lax.optimization_barrier(weights.astype(jnp.bfloat16)).astype(jnp.float32)
        mixture = jnp.einsum('ngqk,nkd->nqgd', rounded, head_values)
        return mixture / jnp.transpose(summed, (0, 2, 1))[..., None]
    stacked = lax.map(window_head, (jnp.moveaxis(query_band, 2, 0), jnp.moveaxis(band_keys, 2, 0), jnp.moveaxis(band_values, 2, 0), sink_table))
    window_out = jnp.moveaxis(stacked, 0, 2).reshape(length_all, HS * HEAD).astype(jnp.bfloat16)
    latent_cols = HM * HEAD // N_TP
    window_cols = HS * HEAD // N_TP
    result = jnp.zeros((length_all, D), jnp.float32)
    for group_index in range(N_TP):
        partial_value = jnp.dot(latent_out[:, group_index * latent_cols:(group_index + 1) * latent_cols], out_latent[group_index * latent_cols:(group_index + 1) * latent_cols], preferred_element_type=jnp.float32)
        partial_value = partial_value + jnp.dot(window_out[:, group_index * window_cols:(group_index + 1) * window_cols], out_window[group_index * window_cols:(group_index + 1) * window_cols], preferred_element_type=jnp.float32)
        result = result + lax.optimization_barrier(partial_value.astype(jnp.bfloat16)).astype(jnp.float32)
    return result.astype(jnp.bfloat16)
```

```python
import functools

import jax
import jax.numpy as jnp
from jax import lax
from jax.experimental import pallas as pl
from jax.experimental.pallas import tpu as pltpu
from jax.sharding import PartitionSpec as P

NOPE = 64
ROPE = 32
HEAD = 64
WINDOW = 128
LOG2E = 1.4426950408889634

MESH = pl.DeviceIdType.MESH
VMEM_LIMIT = 60 * 2**20
Z, Y = 8, 4
BLK = 512
KV_ROWS = BLK + BLK + BLK // 4
HALF = KV_ROWS // 2
O_ROWS = 2 * HEAD + 16


epsilon = 1e-06


def sent_to_all(value, axis):
    peers = lax.axis_size(axis)
    return lax.all_to_all(
        jnp.broadcast_to(value[None], (peers, *value.shape)), axis, 0, 0, tiled=True
    )


def in_order(parts, dim):
    parts = jnp.moveaxis(parts, 0, dim)
    shape = parts.shape
    return parts.reshape(*shape[:dim], shape[dim] * shape[dim + 1], *shape[dim + 2 :])


def gather_directly(value, axis, dim):
    parts = sent_to_all(value, axis)
    return in_order(parts, dim)


def in_blocks(value, dim, peers):
    shape = value.shape
    parts = value.reshape(*shape[:dim], peers, shape[dim] // peers, *shape[dim + 1 :])
    return jnp.moveaxis(parts, dim, 0)


def summed_on_arrival(value, axis, dim):
    parts = in_blocks(value, dim, lax.axis_size(axis))
    arrived = lax.all_to_all(parts, axis, split_axis=0, concat_axis=0, tiled=True)
    return arrived.astype(jnp.float32).sum(axis=0)


def rms_scale(values, gains):
    return values * lax.rsqrt(jnp.mean(values * values, axis=-1, keepdims=True) + epsilon) * gains


def rotary(values, positions):
    half_width = values.shape[-1] // 2
    inverse = 1.0 / 10000.0 ** (
        jnp.arange(0, 2 * half_width, 2).astype(jnp.float32) / (2 * half_width)
    )
    angles = positions[:, None] * inverse[None, :]
    cosine_table = jnp.cos(angles)[:, None, :]
    sine_table = jnp.sin(angles)[:, None, :]
    first_half = values[..., :half_width]
    second_half = values[..., half_width:]
    return jnp.concatenate(
        [
            first_half * cosine_table - second_half * sine_table,
            second_half * cosine_table + first_half * sine_table,
        ],
        axis=-1,
    )


def at_sp(index):
    return {"sp": index}


def split3(value):
    high = value.astype(jnp.bfloat16)
    rest = value - high.astype(jnp.float32)
    middle = rest.astype(jnp.bfloat16)
    low = (rest - middle.astype(jnp.float32)).astype(jnp.bfloat16)
    return high, middle, low


def window_part(wkv, wq_ref, sink_ref, out_ref, sp, length_all):
    values_t = jnp.transpose(wkv[...].astype(jnp.float32))[HEAD:, :].astype(jnp.bfloat16)
    sinks = sink_ref[0:1, :]
    rows = lax.broadcasted_iota(jnp.int32, (3 * WINDOW, 2 * WINDOW), 0)
    cols = lax.broadcasted_iota(jnp.int32, (3 * WINDOW, 2 * WINDOW), 1)
    gap = rows - cols % WINDOW
    near = (gap >= 0) & (gap <= 2 * WINDOW)
    blank = jnp.zeros((HEAD, WINDOW), jnp.bfloat16)
    for n in range(BLK // WINDOW):
        here = slice(n * WINDOW, (n + 1) * WINDOW)
        keys = wkv[n * WINDOW : (n + 3) * WINDOW, :]
        queries = jnp.concatenate(
            [
                jnp.concatenate([wq_ref[0:HEAD, here], blank], axis=0),
                jnp.concatenate([wq_ref[HEAD : 2 * HEAD, here], blank], axis=0),
            ],
            axis=1,
        )
        scores = jnp.dot(keys, queries, preferred_element_type=jnp.float32)
        place = rows + (sp * BLK + (n - 1) * WINDOW)
        allowed = near & (place >= 0) & (place < length_all)
        scores = jnp.where(allowed, scores, -jnp.inf)
        highest = jnp.maximum(jnp.max(scores, axis=0, keepdims=True), sinks)
        weights = jnp.exp2(scores - highest)
        denominators = jnp.sum(weights, axis=0, keepdims=True) + jnp.exp2(sinks - highest)
        mix = jnp.dot(
            values_t[:, n * WINDOW : (n + 3) * WINDOW],
            weights.astype(jnp.bfloat16),
            preferred_element_type=jnp.float32,
        )
        mix = mix / denominators
        both = jnp.concatenate([mix[:, :WINDOW], mix[:, WINDOW:]], axis=0)
        out_ref[here, 2 * HEAD :] = jnp.transpose(both).astype(jnp.bfloat16)


def attention_kernel(
    length_all,
    kv_ref,
    q_ref,
    wkv_ref,
    wq_ref,
    sink_ref,
    out_ref,
    kvs,
    ropes,
    qraw,
    qpad,
    wkv,
    s0,
    s1,
    now_max,
    now_shrink,
    run_max,
    acc,
    o_out,
    o_in,
    kv_send,
    kv_recv,
    q_send,
    q_recv,
    o_send,
    o_recv,
    w_send,
    w_recv,
):
    sp = lax.axis_index("sp")
    z, y = sp // Y, sp % Y
    up = ((z + 1) % Z) * Y + y
    down = ((z + Z - 1) % Z) * Y + y
    right = z * Y + (y + 1) % Y
    left = z * Y + (y + Y - 1) % Y
    across = z * Y + (y + 2) % Y
    after = (sp + 1) % (Z * Y)
    before = (sp + Z * Y - 1) % (Z * Y)
    barrier = pltpu.get_barrier_semaphore()
    peers = (up, down, right, left, across, after, before)
    for peer in peers:
        pl.semaphore_signal(barrier, inc=1, device_id=at_sp(peer), device_id_type=MESH)
    pl.semaphore_wait(barrier, len(peers))

    def copy(src, dst, send, recv, peer):
        return pltpu.make_async_remote_copy(
            src_ref=src,
            dst_ref=dst,
            send_sem=send,
            recv_sem=recv,
            device_id=at_sp(peer),
            device_id_type=MESH,
        )

    def kv_half(ref, half):
        return ref.at[pl.ds(half * HALF, HALF)]

    def kv_copy(step, half, upward):
        came = 0 if step == 1 else (2 * step - 3 if upward else 2 * step - 2)
        goes = 7 if step == 4 else (2 * step - 1 if upward else 2 * step)
        src = kv_half(kv_ref if step == 1 else kvs.at[came], half)
        slot = 2 * goes + half
        return copy(
            src, kv_half(kvs.at[goes], half), kv_send.at[slot], kv_recv.at[slot], up if upward else down
        )

    q_half = q_ref.shape[0] // 2
    q_right = copy(q_ref, qraw.at[1], q_send.at[0], q_recv.at[0], right)
    q_left = copy(q_ref, qraw.at[2], q_send.at[1], q_recv.at[1], left)
    q_on_right = copy(
        qraw.at[1, pl.ds(0, q_half)], qraw.at[3, pl.ds(0, q_half)], q_send.at[2], q_recv.at[2], right
    )
    q_on_left = copy(
        qraw.at[2, pl.ds(q_half, q_half)], qraw.at[3, pl.ds(q_half, q_half)], q_send.at[3], q_recv.at[3], left
    )
    w_after = copy(
        wkv_ref.at[pl.ds(BLK - WINDOW, WINDOW)], wkv.at[pl.ds(0, WINDOW)], w_send.at[0], w_recv.at[0], after
    )
    w_before = copy(
        wkv_ref.at[pl.ds(0, WINDOW)], wkv.at[pl.ds(BLK + WINDOW, WINDOW)], w_send.at[1], w_recv.at[1], before
    )
    w_after.start()
    w_before.start()
    q_right.start()
    q_left.start()
    for half in range(2):
        kv_copy(1, half, True).start()
        kv_copy(1, half, False).start()

    scores_of = (s0, s1)
    blank = jnp.zeros((NOPE, BLK), jnp.bfloat16)

    def set_queries(g, src):
        qpad[2 * g, 0:NOPE] = src[0:NOPE, :]
        qpad[2 * g, NOPE : 2 * NOPE] = blank
        qpad[2 * g + 1, 0:NOPE] = blank
        qpad[2 * g + 1, NOPE : 2 * NOPE] = src[NOPE : 2 * NOPE, :]
        for h in range(2):
            start = 2 * NOPE + h * ROPE
            qpad[2 * g + h, 2 * NOPE : 2 * NOPE + ROPE] = src[start : start + ROPE, :]
            qpad[2 * g + h, 2 * NOPE + ROPE :] = jnp.zeros((128 - ROPE, BLK), jnp.bfloat16)

    def set_ropes(p, packed):
        wide = packed.astype(jnp.float32)
        ropes[p, 0:128] = packed
        for k in range(1, 4):
            ropes[p, 128 * k : 128 * (k + 1)] = pltpu.roll(wide, 128 - 32 * k, 1).astype(jnp.bfloat16)

    def keys_of(p):
        return jnp.concatenate([kvs[p, 0:BLK, :], ropes[p]], axis=1)

    def scores_stage(p, g, h):
        scores = jnp.dot(keys_of(p), qpad[2 * g + h], preferred_element_type=jnp.float32)
        scores_of[h][...] = scores
        before_max = run_max[2 * g + h]
        highest = jnp.maximum(before_max, jnp.max(scores, axis=0, keepdims=True))
        now_shrink[h] = jnp.exp2(before_max - highest)
        now_max[h] = highest
        run_max[2 * g + h] = highest

    def values_stage(p, g, h):
        weights = jnp.exp2(scores_of[h][...] - now_max[h]).astype(jnp.bfloat16)
        values = jnp.concatenate(
            [kvs[p, pl.ds(BLK + 128 * k + HEAD * h, HEAD), :] for k in range(4)], axis=1
        )
        values = jnp.concatenate([values, jnp.ones((16, BLK), jnp.bfloat16)], axis=0)
        mix = jnp.dot(values, weights, preferred_element_type=jnp.float32)
        acc[2 * g + h] = acc[2 * g + h] * now_shrink[h] + mix

    def finish(g, h):
        total = acc[2 * g + h]
        denominator = total[HEAD : HEAD + 1]
        return total[:HEAD] / denominator, run_max[2 * g + h] + jnp.log2(denominator)

    def o_copy(g):
        peer = (None, left, right, across)[g]
        return copy(o_out.at[g - 1], o_in.at[g - 1], o_send.at[g - 1], o_recv.at[g - 1], peer)

    def send_out(g):
        tails = []
        for h in range(2):
            out, level = finish(g, h)
            o_out[g - 1, HEAD * h : HEAD * (h + 1)] = out.astype(jnp.bfloat16)
            tails += [part.astype(jnp.float32) for part in split3(level)]
        tails.append(jnp.zeros((10, BLK), jnp.float32))
        o_out[g - 1, 2 * HEAD :] = jnp.concatenate(tails, axis=0).astype(jnp.bfloat16)
        o_copy(g).start()

    def unit(u):
        w = u - 3
        v = u - 12
        t = u - 24
        k = t // 2
        p = jnp.where(
            u < 3, 0, jnp.where(u < 9, 1 + w // 3, jnp.where(u < 12, u - 9, jnp.where(u < 24, 3 + v // 4, 6 + t % 2)))
        )
        last = jnp.where(k == 0, 3, jnp.where(k == 3, 0, k))
        g = jnp.where(u < 3, u, jnp.where(u < 9, w % 3, jnp.where(u < 12, 3, jnp.where(u < 24, v % 4, last))))
        return p, g

    run_max[...] = jnp.full(run_max.shape, -1e30, jnp.float32)
    acc[...] = jnp.zeros(acc.shape, jnp.float32)
    kvs[0] = kv_ref[...]
    set_queries(0, q_ref)
    set_ropes(0, kv_ref[2 * BLK :, :])
    wkv[WINDOW : WINDOW + BLK, :] = wkv_ref[...]
    w_after.wait()
    w_before.wait()
    window_part(wkv, wq_ref, sink_ref, out_ref, sp, length_all)
    scores_stage(0, 0, 0)

    def arrive(step, half):
        kv_copy(step, half, True).wait_recv()
        kv_copy(step, half, False).wait_recv()

    def at0():
        q_right.wait_recv()
        q_on_right.start()
        q_left.wait_recv()
        q_on_left.start()
        set_queries(1, qraw.at[1])
        set_queries(2, qraw.at[2])

    def at1():
        arrive(1, 0)
        kv_copy(2, 0, True).start()
        kv_copy(2, 0, False).start()

    def at2():
        arrive(1, 1)
        kv_copy(2, 1, True).start()
        kv_copy(2, 1, False).start()
        set_ropes(1, kvs[1, 2 * BLK :, :])
        set_ropes(2, kvs[2, 2 * BLK :, :])

    def at7():
        arrive(2, 0)
        kv_copy(3, 0, True).start()
        kv_copy(3, 0, False).start()

    def at8():
        q_on_right.wait_recv()
        q_on_left.wait_recv()
        set_queries(3, qraw.at[3])

    def at11():
        arrive(2, 1)
        kv_copy(3, 1, True).start()
        kv_copy(3, 1, False).start()
        set_ropes(3, kvs[3, 2 * BLK :, :])
        set_ropes(4, kvs[4, 2 * BLK :, :])

    def at15():
        arrive(3, 0)
        kv_copy(4, 0, True).start()

    def at19():
        arrive(3, 1)
        kv_copy(4, 1, False).start()
        set_ropes(5, kvs[5, 2 * BLK :, :])
        set_ropes(6, kvs[6, 2 * BLK :, :])

    def at24():
        kv_copy(4, 0, True).wait_recv()
        kv_copy(4, 1, False).wait_recv()
        set_ropes(7, kvs[7, 2 * BLK :, :])

    events = {
        0: at0,
        1: at1,
        2: at2,
        7: at7,
        8: at8,
        11: at11,
        15: at15,
        19: at19,
        24: at24,
        26: lambda: send_out(3),
        28: lambda: send_out(1),
        30: lambda: send_out(2),
    }

    def advance(u, carry):
        for when, event in events.items():
            pl.when(u == when)(event)
        p, g = unit(u)
        p_next, g_next = unit(jnp.minimum(u + 1, 31))
        scores_stage(p, g, 1)
        values_stage(p, g, 0)
        scores_stage(p_next, g_next, 0)
        values_stage(p, g, 1)
        return carry

    lax.fori_loop(0, 32, advance, 0)

    own = [finish(0, h) for h in range(2)]
    for g in range(1, 4):
        o_copy(g).wait_recv()
    merged = []
    for h in range(2):
        outs, levels = [own[h][0]], [own[h][1]]
        for g in range(1, 4):
            block = o_in[g - 1].astype(jnp.float32)
            outs.append(block[HEAD * h : HEAD * (h + 1)])
            row = 2 * HEAD + 3 * h
            levels.append(block[row : row + 1] + block[row + 1 : row + 2] + block[row + 2 : row + 3])
        top = functools.reduce(jnp.maximum, levels)
        shares = [jnp.exp2(level - top) for level in levels]
        total = functools.reduce(jnp.add, shares)
        mixed = functools.reduce(jnp.add, [o * (s / total) for o, s in zip(outs, shares)])
        merged.append(mixed)
    out_ref[:, 0 : 2 * HEAD] = jnp.transpose(jnp.concatenate(merged, axis=0)).astype(jnp.bfloat16)

    w_sends = [w_after, w_before, q_right, q_left, q_on_right, q_on_left]
    for step in range(1, 4):
        for half in range(2):
            w_sends += [kv_copy(step, half, True), kv_copy(step, half, False)]
    w_sends += [kv_copy(4, 0, True), kv_copy(4, 1, False)]
    w_sends += [o_copy(g) for g in range(1, 4)]
    for sent in w_sends[2:]:
        sent.wait_send()


def attention(kv, q, wkv, wq, sinks, length_all):
    dma = pltpu.SemaphoreType.DMA
    return pl.pallas_call(
        functools.partial(attention_kernel, length_all),
        out_shape=jax.ShapeDtypeStruct((BLK, 4 * HEAD), jnp.bfloat16),
        in_specs=[pl.BlockSpec(memory_space=pltpu.VMEM)] * 5,
        out_specs=pl.BlockSpec(memory_space=pltpu.VMEM),
        scratch_shapes=[
            pltpu.VMEM((Z, KV_ROWS, 128), jnp.bfloat16),
            pltpu.VMEM((Z, BLK, 128), jnp.bfloat16),
            pltpu.VMEM((Y, 2 * (NOPE + ROPE), BLK), jnp.bfloat16),
            pltpu.VMEM((2 * Y, 256, BLK), jnp.bfloat16),
            pltpu.VMEM((BLK + 2 * WINDOW, 128), jnp.bfloat16),
            pltpu.VMEM((BLK, BLK), jnp.float32),
            pltpu.VMEM((BLK, BLK), jnp.float32),
            pltpu.VMEM((2, 1, BLK), jnp.float32),
            pltpu.VMEM((2, 1, BLK), jnp.float32),
            pltpu.VMEM((2 * Y, 1, BLK), jnp.float32),
            pltpu.VMEM((2 * Y, HEAD + 16, BLK), jnp.float32),
            pltpu.VMEM((Y - 1, O_ROWS, BLK), jnp.bfloat16),
            pltpu.VMEM((Y - 1, O_ROWS, BLK), jnp.bfloat16),
            dma((16,)),
            dma((16,)),
            dma((4,)),
            dma((4,)),
            dma((3,)),
            dma((3,)),
            dma((2,)),
            dma((2,)),
        ],
        compiler_params=pltpu.CompilerParams(
            collective_id=1, has_side_effects=True, vmem_limit_bytes=VMEM_LIMIT
        ),
        name="attention",
    )(kv, q, wkv, wq, sinks)


def shards(
    inputs,
    norm_gain,
    latent_query,
    latent_down,
    rope_down,
    latent_gain,
    latent_up,
    window_query,
    window_key,
    window_value,
    sink_logit,
    out_latent,
    out_window,
):
    row_count = inputs.shape[0]
    gathered = gather_directly(inputs, "tp", 1)
    hidden = rms_scale(gathered.astype(jnp.float32), norm_gain).astype(jnp.bfloat16)
    offset = lax.axis_index("sp") * row_count
    length_all = row_count * lax.axis_size("sp")
    positions = (offset + jnp.arange(row_count)).astype(jnp.float32)
    latent = rms_scale(
        jnp.dot(hidden, latent_down, preferred_element_type=jnp.float32), latent_gain
    ).astype(jnp.bfloat16)
    shared = rotary(
        jnp.dot(hidden, rope_down, preferred_element_type=jnp.float32)[:, None, :], positions
    )[:, 0, :].astype(jnp.bfloat16)
    head_count = latent_up.shape[1] // (NOPE + HEAD)
    queries = jnp.dot(hidden, latent_query, preferred_element_type=jnp.float32).reshape(
        row_count, head_count, NOPE + ROPE
    )
    scale = LOG2E * (NOPE + ROPE) ** (-0.5)
    turned = rotary(queries[..., NOPE:], positions)
    queries_t = (
        jnp.concatenate(
            [
                queries[..., :NOPE].reshape(row_count, head_count * NOPE),
                turned.reshape(row_count, head_count * ROPE),
            ],
            axis=1,
        )
        * scale
    ).T.astype(jnp.bfloat16)
    raising = latent_up.reshape(latent_up.shape[0], head_count, NOPE + HEAD)
    raise_keys = raising[..., :NOPE].reshape(-1, head_count * NOPE)
    raise_values = raising[..., NOPE:].reshape(-1, head_count * HEAD)
    keys = jnp.dot(latent, raise_keys, preferred_element_type=jnp.float32).astype(jnp.bfloat16)
    values_t = lax.dot_general(
        raise_values, latent, (((0,), (1,)), ((), ())), preferred_element_type=jnp.float32
    ).astype(jnp.bfloat16)
    values_t = jnp.swapaxes(values_t.reshape(128, 4, 128), 0, 1).reshape(512, 128)
    packed_rope = jnp.swapaxes(shared.reshape(4, 128, ROPE), 0, 1).reshape(128, 128)
    kv = jnp.concatenate([keys, values_t, packed_rope], axis=0)
    window_heads = window_query.shape[1] // HEAD
    key_heads = window_key.shape[1] // HEAD
    window_queries = rotary(
        jnp.dot(hidden, window_query, preferred_element_type=jnp.float32).reshape(
            row_count, window_heads, HEAD
        ),
        positions,
    )
    queries_w = (
        (window_queries * (LOG2E * HEAD ** (-0.5))).reshape(row_count, window_heads * HEAD).T
    ).astype(jnp.bfloat16)
    window_keys = rotary(
        jnp.dot(hidden, window_key, preferred_element_type=jnp.float32).reshape(
            row_count, key_heads, HEAD
        ),
        positions,
    ).astype(jnp.bfloat16)
    window_values = jnp.dot(hidden, window_value, preferred_element_type=jnp.float32).astype(
        jnp.bfloat16
    )
    packed = jnp.concatenate(
        [window_keys.reshape(row_count, key_heads * HEAD), window_values], axis=1
    )
    sinks = jnp.repeat(sink_logit * LOG2E, WINDOW)[None, :]
    mixed = attention(kv, queries_t, packed, queries_w, sinks, length_all)
    contract_dims = (((0,), (1,)), ((), ()))
    own_rows = summed_on_arrival(
        lax.dot_general(
            jnp.concatenate([out_latent, out_window], axis=0),
            mixed,
            contract_dims,
            preferred_element_type=jnp.float32,
        ).astype(jnp.bfloat16),
        "tp",
        0,
    )
    return jnp.transpose(own_rows).astype(jnp.bfloat16)


def solution(mesh):
    in_specs = (
        P("sp", "tp"),
        P(),
        P(None, "tp"),
        P(),
        P(),
        P(),
        P(None, "tp"),
        P(None, "tp"),
        P(None, "tp"),
        P(None, "tp"),
        P("tp"),
        P("tp", None),
        P("tp", None),
    )
    out_specs = P("sp", "tp")
    return jax.shard_map(shards, mesh=mesh, in_specs=in_specs, out_specs=out_specs, check_vma=False)
```

```python
import functools

import jax
import jax.numpy as jnp
import numpy as np
from jax import lax
from jax.experimental import pallas as pl
from jax.experimental.pallas import tpu as pltpu
from jax.sharding import PartitionSpec as P

NOPE = 64
ROPE = 32
HEAD = 64
WINDOW = 128
LOG2E = 1.4426950408889634

MESH = pl.DeviceIdType.MESH
VMEM_LIMIT = 60 * 2**20
Z, Y, X = 8, 4, 4
BLK = 512
KV_ROWS = BLK + BLK + BLK // 4
HALF = KV_ROWS // 2
O_ROWS = 2 * HEAD + 16
COLS = 256
ROWS = BLK // 2


epsilon = 1e-06


def at_sp(index):
    return {"sp": index}


def split3(value):
    high = value.astype(jnp.bfloat16)
    rest = value - high.astype(jnp.float32)
    middle = rest.astype(jnp.bfloat16)
    low = (rest - middle.astype(jnp.float32)).astype(jnp.bfloat16)
    return high, middle, low


def window_part(wkv, wq_ref, sink_ref, out_ref, sp, length_all):
    values_t = jnp.transpose(wkv[...].astype(jnp.float32))[HEAD:, :].astype(jnp.bfloat16)
    lane = lax.broadcasted_iota(jnp.int32, (1, 2 * WINDOW), 1)
    sinks = jnp.where(lane < WINDOW, sink_ref[0], sink_ref[1]) * LOG2E
    rows = lax.broadcasted_iota(jnp.int32, (3 * WINDOW, 2 * WINDOW), 0)
    cols = lax.broadcasted_iota(jnp.int32, (3 * WINDOW, 2 * WINDOW), 1)
    gap = rows - cols % WINDOW
    near = (gap >= 0) & (gap <= 2 * WINDOW)
    blank = jnp.zeros((HEAD, WINDOW), jnp.bfloat16)
    for n in range(BLK // WINDOW):
        here = slice(n * WINDOW, (n + 1) * WINDOW)
        keys = wkv[n * WINDOW : (n + 3) * WINDOW, :]
        queries = jnp.concatenate(
            [
                jnp.concatenate([wq_ref[0:HEAD, here], blank], axis=0),
                jnp.concatenate([wq_ref[HEAD : 2 * HEAD, here], blank], axis=0),
            ],
            axis=1,
        )
        scores = jnp.dot(keys, queries, preferred_element_type=jnp.float32)
        place = rows + (sp * BLK + (n - 1) * WINDOW)
        allowed = near & (place >= 0) & (place < length_all)
        scores = jnp.where(allowed, scores, -jnp.inf)
        highest = jnp.maximum(jnp.max(scores, axis=0, keepdims=True), sinks)
        weights = jnp.exp2(scores - highest)
        denominators = jnp.sum(weights, axis=0, keepdims=True) + jnp.exp2(sinks - highest)
        mix = jnp.dot(
            values_t[:, n * WINDOW : (n + 3) * WINDOW],
            weights.astype(jnp.bfloat16),
            preferred_element_type=jnp.float32,
        )
        mix = mix / denominators
        both = jnp.concatenate([mix[:, :WINDOW], mix[:, WINDOW:]], axis=0)
        out_ref[here, 2 * HEAD :] = jnp.transpose(both).astype(jnp.bfloat16)


def at_tp(index):
    return {"tp": index}


def remote(src, dst, send, recv, device):
    return pltpu.make_async_remote_copy(
        src_ref=src, dst_ref=dst, send_sem=send, recv_sem=recv, device_id=device, device_id_type=MESH
    )


def turned(rows, half, cosine, sine):
    first, second = rows[:half], rows[half:]
    return [first * cosine - second * sine, second * cosine + first * sine]


def project(
    gain_ref, lgain_ref, near_ref, far_ref, weights, up, kv, q, wkv, wq, xs, squares, accs, x_send, x_recv, ready, raise_ready, send_kv, send_q, send_w
):
    tp = lax.axis_index("tp")
    x, core = tp // 2, tp % 2
    right = ((x + 1) % X) * 2 + core
    left = ((x + X - 1) % X) * 2 + core
    partner = 2 * x + 1 - core

    def half_of(ref, half):
        return ref.at[pl.ds(half * ROWS, ROWS)]

    mine = [2 * r + core for r in range(X)]

    def to_side(half, rightward):
        slot = mine[1] if rightward else mine[3]
        tag = (2 if rightward else 6) + half
        return remote(
            half_of(xs.at[core], half),
            half_of(xs.at[slot], half),
            x_send.at[tag],
            x_recv.at[tag],
            at_tp(right if rightward else left),
        )

    def onward(rightward):
        half = 0 if rightward else 1
        tag = 4 + half
        return remote(
            half_of(xs.at[mine[1] if rightward else mine[3]], half),
            half_of(xs.at[mine[2]], half),
            x_send.at[tag],
            x_recv.at[tag],
            at_tp(right if rightward else left),
        )

    def over(r, half):
        tag = 8 + 2 * r + half
        slot = xs.at[mine[r]]
        return remote(half_of(slot, half), half_of(slot, half), x_send.at[tag], x_recv.at[tag], at_tp(partner))

    own_over = remote(xs.at[core], xs.at[core], x_send.at[0], x_recv.at[0], at_tp(partner))
    to_side(0, True).start()
    to_side(1, False).start()
    own_over.start()
    to_side(1, True).start()
    to_side(0, False).start()
    ready()

    def add(r):
        chip = (x + (0, X - 1, 2, 1)[r]) % X
        values = jnp.concatenate([xs[2 * r], xs[2 * r + 1]], axis=1).astype(jnp.float32)
        square = values * values
        square = square[:, 0:128] + square[:, 128:256] + square[:, 256:384] + square[:, 384:512]
        rows = pl.ds(pl.multiple_of(chip * 2 * COLS, 2 * COLS), 2 * COLS)
        scaled = (values * gain_ref[:, rows]).astype(jnp.bfloat16)
        if r == 0:
            squares[...] = square
        else:
            squares[...] += square
        slim = lax.dot_general(
            weights[0][:, rows], scaled, (((1,), (1,)), ((), ())), preferred_element_type=jnp.float32
        )
        products = [slim] + [
            jnp.dot(scaled, weight[rows, :], preferred_element_type=jnp.float32) for weight in weights[1:]
        ]
        for product, acc in zip(products, accs):
            if r == 0:
                acc[...] = product
            else:
                acc[...] += product

    own_over.wait_recv()
    add(0)
    to_side(0, True).wait_recv()
    onward(True).start()
    over(1, 0).start()
    to_side(1, False).wait_recv()
    onward(False).start()
    over(3, 1).start()
    to_side(1, True).wait_recv()
    over(1, 1).start()
    to_side(0, False).wait_recv()
    over(3, 0).start()
    for half in range(2):
        over(1, half).wait_recv()
    add(1)
    for half in range(2):
        over(3, half).wait_recv()
    add(3)
    onward(True).wait_recv()
    over(2, 0).start()
    onward(False).wait_recv()
    over(2, 1).start()
    for half in range(2):
        over(2, half).wait_recv()
    add(2)

    width = 2 * COLS * X
    scale = lax.rsqrt(jnp.sum(squares[...], axis=1, keepdims=True) / width + epsilon)
    acc_slim, acc_ld, acc_wq = accs
    row_scale = lax.rsqrt(jnp.sum(jnp.transpose(squares[...]), axis=0, keepdims=True) / width + epsilon)
    turn = far_ref[...]
    here = lax.broadcasted_iota(jnp.int32, turn.shape, 2) == lax.axis_index("sp")
    turn = jnp.sum(jnp.where(here, turn, 0.0), axis=2, keepdims=True)
    far_cos, far_sin = turn[0], turn[1]
    near_cos, near_sin = near_ref[0], near_ref[1]
    cosine = far_cos * near_cos - far_sin * near_sin
    sine = far_sin * near_cos + far_cos * near_sin
    wide_cos, wide_sin = cosine[0:32], sine[0:32]
    slim_cos, slim_sin = cosine[32:48], sine[32:48]
    mixed = acc_slim[0 : SLIM[2]] * row_scale
    keys = jnp.concatenate(turned(mixed[SLIM[0] : SLIM[1]], HEAD // 2, wide_cos, wide_sin), axis=0)
    values_t = mixed[SLIM[1] : SLIM[2]]
    wkv[...] = jnp.transpose(jnp.concatenate([keys, values_t], axis=0)).astype(jnp.bfloat16)
    send_w()
    sharp = LOG2E * (NOPE + ROPE) ** (-0.5)
    wide = NOPE + ROPE
    pieces = [mixed[0:NOPE], mixed[wide : wide + NOPE]]
    for h in range(2):
        pieces += turned(mixed[wide * h + NOPE : wide * (h + 1)], ROPE // 2, slim_cos, slim_sin)
    q[...] = (jnp.concatenate(pieces, axis=0) * sharp).astype(jnp.bfloat16)
    send_q()
    raise_ready()
    low = acc_ld[...] * scale
    low = low * lax.rsqrt(jnp.mean(low * low, axis=1, keepdims=True) + epsilon) * lgain_ref[0:1, :]
    expanded = jnp.dot(low.astype(jnp.bfloat16), up[...], preferred_element_type=jnp.float32)
    lane = lax.broadcasted_iota(jnp.int32, (BLK, 128), 1)
    one, two = expanded[:, 0:128], expanded[:, 128:256]
    kv[0:BLK, :] = jnp.where(lane < HEAD, one, pltpu.roll(two, HEAD, 1)).astype(jnp.bfloat16)
    values = jnp.where(lane < HEAD, pltpu.roll(one, HEAD, 1), two)
    for k in range(4):
        block = slice(BLK + 128 * k, BLK + 128 * (k + 1))
        kv[block, :] = jnp.transpose(values[128 * k : 128 * (k + 1)]).astype(jnp.bfloat16)
    shared = acc_slim[SLIM[2] : SLIM[3]] * row_scale
    shared = jnp.concatenate(turned(shared, ROPE // 2, slim_cos, slim_sin), axis=0)
    packed = jnp.concatenate([shared[:, 128 * k : 128 * (k + 1)] for k in range(4)], axis=0)
    kv[2 * BLK :, :] = jnp.transpose(packed).astype(jnp.bfloat16)
    send_kv()
    queries = jnp.transpose(acc_wq[...] * scale)
    pieces = []
    for h in range(2):
        pieces += turned(queries[HEAD * h : HEAD * (h + 1)], HEAD // 2, wide_cos, wide_sin)
    wq[...] = (jnp.concatenate(pieces, axis=0) * (LOG2E * HEAD ** (-0.5))).astype(jnp.bfloat16)

    sent = [own_over, onward(True), onward(False)]
    sent += [to_side(half, way) for half in range(2) for way in (True, False)]
    sent += [over(r, half) for r in (1, 2, 3) for half in range(2)]
    return sent


def reduce(mixed, wl, ww, out_ref, pair_out, pair_in, passed, gone, kept, side_out, side_in, r_send, r_recv):
    tp = lax.axis_index("tp")
    x, core = tp // 2, tp % 2
    right = ((x + 1) % X) * 2 + core
    left = ((x + X - 1) % X) * 2 + core
    partner = 2 * x + 1 - core
    values = mixed[...]

    def projected(r, core_to):
        block = ((x + r) % X) * 2 + core_to
        cols = pl.ds(pl.multiple_of(block * COLS, COLS), COLS)
        weight = jnp.concatenate([wl[:, cols], ww[:, cols]], axis=0)
        return jnp.dot(values, weight, preferred_element_type=jnp.float32)

    def pair(r):
        return remote(pair_out.at[r], pair_in.at[r], r_send.at[r], r_recv.at[r], at_tp(partner))

    def far(half):
        return remote(
            gone.at[half], passed.at[half], r_send.at[4 + half], r_recv.at[4 + half], at_tp((right, left)[half])
        )

    def side(rightward, half):
        tag = 2 * (0 if rightward else 1) + half
        return remote(
            side_out.at[tag], side_in.at[tag], r_send.at[6 + tag], r_recv.at[6 + tag], at_tp(right if rightward else left)
        )

    def start_pair(r):
        pair_out[r] = projected(r, 1 - core).astype(jnp.bfloat16)
        pair(r).start()

    order = (2, 1, 3, 0)
    start_pair(2)
    own_next = projected(2, core)
    start_pair(1)
    for n, r in enumerate(order):
        own = own_next
        pair(r).wait_recv()
        total = own + pair_in[r].astype(jnp.float32)
        upper, lower = total[:ROWS], total[ROWS:]
        if r == 2:
            gone[0] = upper.astype(jnp.bfloat16)
            far(0).start()
            gone[1] = lower.astype(jnp.bfloat16)
            far(1).start()
        elif r == 1:
            side_out[1] = lower.astype(jnp.bfloat16)
            side(True, 1).start()
            kept[0] = upper
        elif r == 3:
            side_out[2] = upper.astype(jnp.bfloat16)
            side(False, 0).start()
            kept[1] = lower
        else:
            kept[2] = upper
            kept[3] = lower
        if n < 2:
            start_pair(order[n + 2])
        if n < 3:
            own_next = projected(order[n + 1], core)
    far(0).wait_recv()
    side_out[0] = (kept[0] + passed[0].astype(jnp.float32)).astype(jnp.bfloat16)
    side(True, 0).start()
    far(1).wait_recv()
    side_out[3] = (kept[1] + passed[1].astype(jnp.float32)).astype(jnp.bfloat16)
    side(False, 1).start()
    for half in (1, 0):
        side(True, half).wait_recv()
        side(False, half).wait_recv()
    for half in range(2):
        total = kept[2 + half] + side_in[half].astype(jnp.float32) + side_in[2 + half].astype(jnp.float32)
        out_ref[half * ROWS : (half + 1) * ROWS, :] = total.astype(jnp.bfloat16)
    sent = [pair(r) for r in range(X)] + [far(half) for half in range(2)]
    return sent + [side(way, half) for way in (True, False) for half in range(2)]


SLIM = (192, 256, 320, 352)


def layer_kernel(
    length_all,
    sink_ref,
    x_hbm,
    gain_hbm,
    lgain_hbm,
    near_hbm,
    far_hbm,
    lq_hbm,
    wk_hbm,
    wv_hbm,
    rd_hbm,
    ld_hbm,
    wq_hbm,
    up_hbm,
    ol_hbm,
    ow_hbm,
    result_ref,
    gain_ref,
    lgain_ref,
    near_ref,
    far_ref,
    w_slim,
    w_ld,
    w_wq,
    w_up,
    w_ol,
    w_ow,
    xs,
    squares,
    a_slim,
    a_ld,
    a_wq,
    kv_ref,
    q_ref,
    wkv_ref,
    wq_ref,
    out_ref,
    kvs,
    ropes,
    qraw,
    qpad,
    wkv,
    s0,
    s1,
    now_max,
    now_shrink,
    run_max,
    acc,
    o_out,
    o_in,
    pair_out,
    pair_in,
    passed,
    gone,
    kept,
    side_out,
    side_in,
    load_sem,
    x_send,
    x_recv,
    kv_send,
    kv_recv,
    q_send,
    q_recv,
    o_send,
    o_recv,
    w_send,
    w_recv,
    r_send,
    r_recv,
):
    sp = lax.axis_index("sp")
    z, y = sp // Y, sp % Y
    up = ((z + 1) % Z) * Y + y
    down = ((z + Z - 1) % Z) * Y + y
    right = z * Y + (y + 1) % Y
    left = z * Y + (y + Y - 1) % Y
    across = z * Y + (y + 2) % Y
    after = (sp + 1) % (Z * Y)
    before = (sp + Z * Y - 1) % (Z * Y)
    barrier = pltpu.get_barrier_semaphore()
    peers = [at_sp(peer) for peer in (up, down, right, left, across, after, before)]
    tp = lax.axis_index("tp")
    x, core = tp // 2, tp % 2
    peers += [at_tp((tp + 2) % (2 * X)), at_tp((tp + 2 * X - 2) % (2 * X)), at_tp(2 * x + 1 - core)]
    for peer in peers:
        pl.semaphore_signal(barrier, inc=1, device_id=peer, device_id_type=MESH)
    load_x = pltpu.make_async_copy(x_hbm, xs.at[core], load_sem.at[13])
    load_x.start()
    sources = (gain_hbm, lgain_hbm, near_hbm, far_hbm, lq_hbm, wk_hbm, wv_hbm, rd_hbm, ld_hbm, wq_hbm, up_hbm, ol_hbm, ow_hbm)
    ends = (0, *SLIM)
    targets = [gain_ref, lgain_ref, near_ref, far_ref]
    targets += [w_slim.at[pl.ds(a, b - a)] for a, b in zip(ends, SLIM)] + [w_ld, w_wq, w_up, w_ol, w_ow]
    loads = [
        pltpu.make_async_copy(source, target, load_sem.at[n])
        for n, (source, target) in enumerate(zip(sources, targets))
    ]
    for load in loads:
        load.start()
    load_x.wait()
    pl.semaphore_wait(barrier, len(peers))

    def copy(src, dst, send, recv, peer):
        return pltpu.make_async_remote_copy(
            src_ref=src,
            dst_ref=dst,
            send_sem=send,
            recv_sem=recv,
            device_id=at_sp(peer),
            device_id_type=MESH,
        )

    def kv_half(ref, half):
        return ref.at[pl.ds(half * HALF, HALF)]

    def kv_copy(step, half, upward):
        came = 0 if step == 1 else (2 * step - 3 if upward else 2 * step - 2)
        goes = 7 if step == 4 else (2 * step - 1 if upward else 2 * step)
        src = kv_half(kv_ref if step == 1 else kvs.at[came], half)
        slot = 2 * goes + half
        return copy(
            src, kv_half(kvs.at[goes], half), kv_send.at[slot], kv_recv.at[slot], up if upward else down
        )

    q_half = q_ref.shape[0] // 2
    q_right = copy(q_ref, qraw.at[1], q_send.at[0], q_recv.at[0], right)
    q_left = copy(q_ref, qraw.at[2], q_send.at[1], q_recv.at[1], left)
    q_on_right = copy(
        qraw.at[1, pl.ds(0, q_half)], qraw.at[3, pl.ds(0, q_half)], q_send.at[2], q_recv.at[2], right
    )
    q_on_left = copy(
        qraw.at[2, pl.ds(q_half, q_half)], qraw.at[3, pl.ds(q_half, q_half)], q_send.at[3], q_recv.at[3], left
    )
    w_after = copy(
        wkv_ref.at[pl.ds(BLK - WINDOW, WINDOW)], wkv.at[pl.ds(0, WINDOW)], w_send.at[0], w_recv.at[0], after
    )
    w_before = copy(
        wkv_ref.at[pl.ds(0, WINDOW)], wkv.at[pl.ds(BLK + WINDOW, WINDOW)], w_send.at[1], w_recv.at[1], before
    )

    def load_weights():
        run_max[...] = jnp.full(run_max.shape, -1e30, jnp.float32)
        acc[...] = jnp.zeros(acc.shape, jnp.float32)
        for load in loads[:-3]:
            load.wait()

    def send_kv():
        for load in loads[-2:]:
            load.wait()
        for half in range(2):
            kv_copy(1, half, True).start()
            kv_copy(1, half, False).start()

    def send_q():
        q_right.start()
        q_left.start()

    def send_w():
        w_after.start()
        w_before.start()

    x_sent = project(
        gain_ref,
        lgain_ref,
        near_ref,
        far_ref,
        (w_slim, w_ld, w_wq),
        w_up,
        kv_ref,
        q_ref,
        wkv_ref,
        wq_ref,
        xs,
        squares,
        (a_slim, a_ld, a_wq),
        x_send,
        x_recv,
        load_weights,
        loads[-3].wait,
        send_kv,
        send_q,
        send_w,
    )

    scores_of = (s0, s1)
    blank = jnp.zeros((NOPE, BLK), jnp.bfloat16)

    def set_queries(g, src):
        qpad[2 * g, 0:NOPE] = src[0:NOPE, :]
        qpad[2 * g, NOPE : 2 * NOPE] = blank
        qpad[2 * g + 1, 0:NOPE] = blank
        qpad[2 * g + 1, NOPE : 2 * NOPE] = src[NOPE : 2 * NOPE, :]
        for h in range(2):
            start = 2 * NOPE + h * ROPE
            qpad[2 * g + h, 2 * NOPE : 2 * NOPE + ROPE] = src[start : start + ROPE, :]
            qpad[2 * g + h, 2 * NOPE + ROPE :] = jnp.zeros((128 - ROPE, BLK), jnp.bfloat16)

    def set_ropes(p, packed):
        wide = packed.astype(jnp.float32)
        ropes[p, 0:128] = packed
        for k in range(1, 4):
            ropes[p, 128 * k : 128 * (k + 1)] = pltpu.roll(wide, 128 - 32 * k, 1).astype(jnp.bfloat16)

    def keys_of(p):
        return jnp.concatenate([kvs[p, 0:BLK, :], ropes[p]], axis=1)

    def scores_stage(p, g, h):
        scores = jnp.dot(keys_of(p), qpad[2 * g + h], preferred_element_type=jnp.float32)
        scores_of[h][...] = scores
        before_max = run_max[2 * g + h]
        highest = jnp.maximum(before_max, jnp.max(scores, axis=0, keepdims=True))
        now_shrink[h] = jnp.exp2(before_max - highest)
        now_max[h] = highest
        run_max[2 * g + h] = highest

    def values_stage(p, g, h):
        weights = jnp.exp2(scores_of[h][...] - now_max[h]).astype(jnp.bfloat16)
        values = jnp.concatenate(
            [kvs[p, pl.ds(BLK + 128 * k + HEAD * h, HEAD), :] for k in range(4)], axis=1
        )
        values = jnp.concatenate([values, jnp.ones((16, BLK), jnp.bfloat16)], axis=0)
        mix = jnp.dot(values, weights, preferred_element_type=jnp.float32)
        acc[2 * g + h] = acc[2 * g + h] * now_shrink[h] + mix

    def finish(g, h):
        total = acc[2 * g + h]
        denominator = total[HEAD : HEAD + 1]
        return total[:HEAD] / denominator, run_max[2 * g + h] + jnp.log2(denominator)

    def o_copy(g):
        peer = (None, left, right, across)[g]
        return copy(o_out.at[g - 1], o_in.at[g - 1], o_send.at[g - 1], o_recv.at[g - 1], peer)

    def send_out(g):
        tails = []
        for h in range(2):
            out, level = finish(g, h)
            o_out[g - 1, HEAD * h : HEAD * (h + 1)] = out.astype(jnp.bfloat16)
            tails += [part.astype(jnp.float32) for part in split3(level)]
        tails.append(jnp.zeros((10, BLK), jnp.float32))
        o_out[g - 1, 2 * HEAD :] = jnp.concatenate(tails, axis=0).astype(jnp.bfloat16)
        o_copy(g).start()

    def unit(u):
        p, g = jnp.where(u < 3, 0, 1 + (u - 3) // 2), jnp.where(u < 3, u, 1 + (u - 3) % 2)
        p, g = jnp.where(u < 7, p, u - 7), jnp.where(u < 7, g, 3)
        p, g = jnp.where(u < 10, p, 3 + (u - 10) // 4), jnp.where(u < 10, g, (u - 10) % 4)
        p, g = jnp.where(u < 18, p, 5 + (u - 18) // 3), jnp.where(u < 18, g, 3 - (u - 18) % 3)
        p = jnp.where(u < 27, p, jnp.where(u < 29, u - 26, u - 24))
        g = jnp.where(u < 27, g, 0)
        return p, g

    kvs[0] = kv_ref[...]
    set_queries(0, q_ref)
    set_ropes(0, kv_ref[2 * BLK :, :])
    wkv[WINDOW : WINDOW + BLK, :] = wkv_ref[...]
    w_after.wait_recv()
    w_before.wait_recv()
    window_part(wkv, wq_ref, sink_ref, out_ref, sp, length_all)
    scores_stage(0, 0, 0)

    def arrive(step, half):
        kv_copy(step, half, True).wait_recv()
        kv_copy(step, half, False).wait_recv()

    def at0():
        q_right.wait_recv()
        q_on_right.start()
        q_left.wait_recv()
        q_on_left.start()
        set_queries(1, qraw.at[1])
        set_queries(2, qraw.at[2])

    def at1():
        arrive(1, 0)
        kv_copy(2, 0, True).start()
        kv_copy(2, 0, False).start()

    def at2():
        arrive(1, 1)
        kv_copy(2, 1, True).start()
        kv_copy(2, 1, False).start()
        set_ropes(1, kvs[1, 2 * BLK :, :])
        set_ropes(2, kvs[2, 2 * BLK :, :])

    def at5():
        arrive(2, 0)
        kv_copy(3, 0, True).start()
        kv_copy(3, 0, False).start()

    def at6():
        q_on_right.wait_recv()
        q_on_left.wait_recv()
        set_queries(3, qraw.at[3])

    def at9():
        arrive(2, 1)
        kv_copy(3, 1, True).start()
        kv_copy(3, 1, False).start()
        set_ropes(3, kvs[3, 2 * BLK :, :])
        set_ropes(4, kvs[4, 2 * BLK :, :])

    def at13():
        arrive(3, 0)
        kv_copy(4, 0, True).start()

    def at17():
        arrive(3, 1)
        kv_copy(4, 1, False).start()
        set_ropes(5, kvs[5, 2 * BLK :, :])
        set_ropes(6, kvs[6, 2 * BLK :, :])

    def at23():
        kv_copy(4, 0, True).wait_recv()
        kv_copy(4, 1, False).wait_recv()
        set_ropes(7, kvs[7, 2 * BLK :, :])

    events = {
        0: at0,
        1: at1,
        2: at2,
        5: at5,
        6: at6,
        9: at9,
        13: at13,
        17: at17,
        23: at23,
        25: lambda: send_out(3),
        26: lambda: send_out(2),
        27: lambda: send_out(1),
    }

    def advance(u, carry):
        for when, event in events.items():
            pl.when(u == when)(event)
        p, g = unit(u)
        p_next, g_next = unit(jnp.minimum(u + 1, 31))
        scores_stage(p, g, 1)
        values_stage(p, g, 0)
        scores_stage(p_next, g_next, 0)
        values_stage(p, g, 1)
        return carry

    lax.fori_loop(0, 32, advance, 0)

    own = [finish(0, h) for h in range(2)]
    for g in range(1, 4):
        o_copy(g).wait_recv()
    merged = []
    for h in range(2):
        outs, levels = [own[h][0]], [own[h][1]]
        for g in range(1, 4):
            block = o_in[g - 1].astype(jnp.float32)
            outs.append(block[HEAD * h : HEAD * (h + 1)])
            row = 2 * HEAD + 3 * h
            levels.append(block[row : row + 1] + block[row + 1 : row + 2] + block[row + 2 : row + 3])
        top = functools.reduce(jnp.maximum, levels)
        shares = [jnp.exp2(level - top) for level in levels]
        total = functools.reduce(jnp.add, shares)
        mixed = functools.reduce(jnp.add, [o * (s / total) for o, s in zip(outs, shares)])
        merged.append(mixed)
    out_ref[:, 0 : 2 * HEAD] = jnp.transpose(jnp.concatenate(merged, axis=0)).astype(jnp.bfloat16)

    r_sent = reduce(
        out_ref, w_ol, w_ow, result_ref, pair_out, pair_in, passed, gone, kept, side_out, side_in, r_send, r_recv
    )

    w_sends = [w_after, w_before, q_right, q_left, q_on_right, q_on_left]
    for step in range(1, 4):
        for half in range(2):
            w_sends += [kv_copy(step, half, True), kv_copy(step, half, False)]
    w_sends += [kv_copy(4, 0, True), kv_copy(4, 1, False)]
    w_sends += [o_copy(g) for g in range(1, 4)]
    for sent in w_sends + x_sent + r_sent:
        sent.wait_send()


def tables():
    near, freqs = [], []
    for width in (HEAD, ROPE):
        half = width // 2
        freqs.append(10000.0 ** (-np.arange(half) / half))
    freqs = np.concatenate(freqs)
    angles = freqs[:, None] * np.arange(BLK)[None, :]
    near = np.stack([np.cos(angles), np.sin(angles)]).astype(np.float32)
    angles = freqs[:, None] * (BLK * np.arange(128))[None, :]
    far = np.stack([np.cos(angles), np.sin(angles)]).astype(np.float32)
    return near, far


def shards(
    inputs,
    norm_gain,
    latent_query,
    latent_down,
    rope_down,
    latent_gain,
    latent_up,
    window_query,
    window_key,
    window_value,
    sink_logit,
    out_latent,
    out_window,
):
    length_all = BLK * Z * Y
    near, far = tables()
    dma = pltpu.SemaphoreType.DMA
    bf16, f32 = jnp.bfloat16, jnp.float32
    in_vmem = pl.BlockSpec(memory_space=pltpu.VMEM)
    in_smem = pl.BlockSpec(memory_space=pltpu.SMEM)
    in_hbm = pl.BlockSpec(memory_space=pltpu.HBM)
    rows = norm_gain.shape[0]
    return pl.pallas_call(
        functools.partial(layer_kernel, length_all),
        out_shape=jax.ShapeDtypeStruct((BLK, COLS), bf16),
        in_specs=[in_smem] + [in_hbm] * 14,
        out_specs=in_vmem,
        scratch_shapes=[
            pltpu.VMEM((1, rows), f32),
            pltpu.VMEM((1, latent_gain.shape[0]), f32),
            pltpu.VMEM(near.shape, f32),
            pltpu.VMEM(far.shape, f32),
            pltpu.VMEM((SLIM[3], rows), bf16),
            pltpu.VMEM(latent_down.shape, bf16),
            pltpu.VMEM(window_query.shape, bf16),
            pltpu.VMEM(latent_up.shape, bf16),
            pltpu.VMEM(out_latent.shape, bf16),
            pltpu.VMEM(out_window.shape, bf16),
            pltpu.VMEM((2 * X, BLK, COLS), bf16),
            pltpu.VMEM((BLK, 128), f32),
            pltpu.VMEM((SLIM[3], BLK), f32),
            pltpu.VMEM((BLK, latent_down.shape[1]), f32),
            pltpu.VMEM((BLK, window_query.shape[1]), f32),
            pltpu.VMEM((KV_ROWS, 128), bf16),
            pltpu.VMEM((2 * (NOPE + ROPE), BLK), bf16),
            pltpu.VMEM((BLK, 2 * HEAD), bf16),
            pltpu.VMEM((2 * HEAD, BLK), bf16),
            pltpu.VMEM((BLK, 4 * HEAD), bf16),
            pltpu.VMEM((Z, KV_ROWS, 128), bf16),
            pltpu.VMEM((Z, BLK, 128), bf16),
            pltpu.VMEM((Y, 2 * (NOPE + ROPE), BLK), bf16),
            pltpu.VMEM((2 * Y, 256, BLK), bf16),
            pltpu.VMEM((BLK + 2 * WINDOW, 128), bf16),
            pltpu.VMEM((BLK, BLK), f32),
            pltpu.VMEM((BLK, BLK), f32),
            pltpu.VMEM((2, 1, BLK), f32),
            pltpu.VMEM((2, 1, BLK), f32),
            pltpu.VMEM((2 * Y, 1, BLK), f32),
            pltpu.VMEM((2 * Y, HEAD + 16, BLK), f32),
            pltpu.VMEM((Y - 1, O_ROWS, BLK), bf16),
            pltpu.VMEM((Y - 1, O_ROWS, BLK), bf16),
            pltpu.VMEM((X, BLK, COLS), bf16),
            pltpu.VMEM((X, BLK, COLS), bf16),
            pltpu.VMEM((2, ROWS, COLS), bf16),
            pltpu.VMEM((2, ROWS, COLS), bf16),
            pltpu.VMEM((4, ROWS, COLS), f32),
            pltpu.VMEM((4, ROWS, COLS), bf16),
            pltpu.VMEM((4, ROWS, COLS), bf16),
            dma((14,)),
            dma((16,)),
            dma((16,)),
            dma((16,)),
            dma((16,)),
            dma((4,)),
            dma((4,)),
            dma((3,)),
            dma((3,)),
            dma((2,)),
            dma((2,)),
            dma((10,)),
            dma((10,)),
        ],
        compiler_params=pltpu.CompilerParams(
            collective_id=1, has_side_effects=True, vmem_limit_bytes=VMEM_LIMIT
        ),
        name="layer",
    )(
        sink_logit,
        inputs,
        norm_gain[None, :],
        latent_gain[None, :],
        near,
        far,
        latent_query.T,
        window_key.T,
        window_value.T,
        rope_down.T,
        latent_down,
        window_query,
        latent_up,
        out_latent,
        out_window,
    )


def solution(mesh):
    in_specs = (
        P("sp", "tp"),
        P(),
        P(None, "tp"),
        P(),
        P(),
        P(),
        P(None, "tp"),
        P(None, "tp"),
        P(None, "tp"),
        P(None, "tp"),
        P("tp"),
        P("tp", None),
        P("tp", None),
    )
    out_specs = P("sp", "tp")
    return jax.shard_map(shards, mesh=mesh, in_specs=in_specs, out_specs=out_specs, check_vma=False)
```

```python
import functools

import jax
import jax.numpy as jnp
import numpy as np
from jax import lax
from jax.experimental import pallas as pl
from jax.experimental.pallas import tpu as pltpu
from jax.sharding import PartitionSpec as P

NOPE = 64
ROPE = 32
HEAD = 64
WINDOW = 128
LOG2E = 1.4426950408889634

MESH = pl.DeviceIdType.MESH
VMEM_LIMIT = 60 * 2**20
Z, Y, X = 8, 4, 4
BLK = 512
HALF = BLK // 2 + BLK // 2 + BLK // 8
O_ROWS = 2 * HEAD + 16
COLS = 256
ROWS = BLK // 2
QUARTER = BLK // 4
TILE = 256
PAIRS = Y * Z // 2


epsilon = 1e-06


def at_sp(index):
    return {"sp": index}


def split3(value):
    high = value.astype(jnp.bfloat16)
    rest = value - high.astype(jnp.float32)
    middle = rest.astype(jnp.bfloat16)
    low = (rest - middle.astype(jnp.float32)).astype(jnp.bfloat16)
    return high, middle, low


def window_part(wkv, wq_ref, sink_ref, out_ref, sp, length_all):
    values_t = jnp.transpose(wkv[...].astype(jnp.float32))[HEAD:, :].astype(jnp.bfloat16)
    lane = lax.broadcasted_iota(jnp.int32, (1, 2 * WINDOW), 1)
    sinks = jnp.where(lane < WINDOW, sink_ref[0], sink_ref[1]) * LOG2E
    rows = lax.broadcasted_iota(jnp.int32, (3 * WINDOW, 2 * WINDOW), 0)
    cols = lax.broadcasted_iota(jnp.int32, (3 * WINDOW, 2 * WINDOW), 1)
    gap = rows - cols % WINDOW
    near = (gap >= 0) & (gap <= 2 * WINDOW)
    blank = jnp.zeros((HEAD, WINDOW), jnp.bfloat16)
    for n in range(BLK // WINDOW):
        here = slice(n * WINDOW, (n + 1) * WINDOW)
        keys = wkv[n * WINDOW : (n + 3) * WINDOW, :]
        queries = jnp.concatenate(
            [
                jnp.concatenate([wq_ref[0:HEAD, here], blank], axis=0),
                jnp.concatenate([wq_ref[HEAD : 2 * HEAD, here], blank], axis=0),
            ],
            axis=1,
        )
        scores = jnp.dot(keys, queries, preferred_element_type=jnp.float32)
        place = rows + (sp * BLK + (n - 1) * WINDOW)
        allowed = near & (place >= 0) & (place < length_all)
        scores = jnp.where(allowed, scores, -jnp.inf)
        highest = jnp.maximum(jnp.max(scores, axis=0, keepdims=True), sinks)
        weights = jnp.exp2(scores - highest)
        denominators = jnp.sum(weights, axis=0, keepdims=True) + jnp.exp2(sinks - highest)
        mix = jnp.dot(
            values_t[:, n * WINDOW : (n + 3) * WINDOW],
            weights.astype(jnp.bfloat16),
            preferred_element_type=jnp.float32,
        )
        mix = mix / denominators
        both = jnp.concatenate([mix[:, :WINDOW], mix[:, WINDOW:]], axis=0)
        out_ref[here, 2 * HEAD :] = jnp.transpose(both).astype(jnp.bfloat16)


def at_tp(index):
    return {"tp": index}


def remote(src, dst, send, recv, device):
    return pltpu.make_async_remote_copy(
        src_ref=src, dst_ref=dst, send_sem=send, recv_sem=recv, device_id=device, device_id_type=MESH
    )


def turned(rows, half, cosine, sine):
    first, second = rows[:half], rows[half:]
    return [first * cosine - second * sine, second * cosine + first * sine]


def project(
    gain_ref, lgain_ref, near_ref, far_ref, weights, up, kv, q, wkv, wq, xs, squares, accs, x_send, x_recv, ready, raise_ready, send_kv, send_q, send_w
):
    tp = lax.axis_index("tp")
    x, core = tp // 2, tp % 2
    right = ((x + 1) % X) * 2 + core
    left = ((x + X - 1) % X) * 2 + core
    partner = 2 * x + 1 - core

    def rows_of(ref, start, size):
        return ref.at[pl.ds(start, size)]

    mine = [2 * r + core for r in range(X)]

    def to_side(quarter, rightward):
        slot = mine[1] if rightward else mine[3]
        tag = quarter + (0 if rightward else 4)
        return remote(
            rows_of(xs.at[core], quarter * QUARTER, QUARTER),
            rows_of(xs.at[slot], quarter * QUARTER, QUARTER),
            x_send.at[tag],
            x_recv.at[tag],
            at_tp(right if rightward else left),
        )

    def onward(half, rightward):
        start = half * ROWS + (0 if rightward else QUARTER)
        tag = 8 + 2 * half + (0 if rightward else 1)
        return remote(
            rows_of(xs.at[mine[1] if rightward else mine[3]], start, QUARTER),
            rows_of(xs.at[mine[2]], start, QUARTER),
            x_send.at[tag],
            x_recv.at[tag],
            at_tp(right if rightward else left),
        )

    def over(r, half):
        tag = 12 + 2 * r + half
        slot = rows_of(xs.at[mine[r]], half * ROWS, ROWS)
        return remote(slot, slot, x_send.at[tag], x_recv.at[tag], at_tp(partner))

    for quarter in (0, 1, 2):
        to_side(quarter, True).start()
        to_side((1, 0, 3)[quarter], False).start()
    over(0, 0).start()
    over(0, 1).start()
    ready()

    def add(r, half):
        chip = (x + (0, X - 1, 2, 1)[r]) % X
        here = slice(half * ROWS, (half + 1) * ROWS)
        values = jnp.concatenate([xs[2 * r, here], xs[2 * r + 1, here]], axis=1).astype(jnp.float32)
        square = values * values
        square = square[:, 0:128] + square[:, 128:256] + square[:, 256:384] + square[:, 384:512]
        rows = pl.ds(pl.multiple_of(chip * 2 * COLS, 2 * COLS), 2 * COLS)
        scaled = (values * gain_ref[:, rows]).astype(jnp.bfloat16)
        slim = lax.dot_general(
            weights[0][:, rows], scaled, (((1,), (1,)), ((), ())), preferred_element_type=jnp.float32
        )
        wide = [jnp.dot(scaled, weight[rows, :], preferred_element_type=jnp.float32) for weight in weights[1:]]
        if r == 0:
            squares[here, :] = square
            accs[0][:, here] = slim
            for product, acc in zip(wide, accs[1:]):
                acc[here, :] = product
        else:
            squares[here, :] += square
            accs[0][:, here] += slim
            for product, acc in zip(wide, accs[1:]):
                acc[here, :] += product

    width = 2 * COLS * X
    acc_slim, acc_ld, acc_wq = accs
    turn = far_ref[...]
    here = lax.broadcasted_iota(jnp.int32, turn.shape, 2) == lax.axis_index("sp")
    turn = jnp.sum(jnp.where(here, turn, 0.0), axis=2, keepdims=True)
    far_cos, far_sin = turn[0], turn[1]
    near_cos, near_sin = near_ref[0], near_ref[1]
    cosine = far_cos * near_cos - far_sin * near_sin
    sine = far_sin * near_cos + far_cos * near_sin
    wide_cos, wide_sin = cosine[0:32], sine[0:32]
    slim_cos, slim_sin = cosine[32:48], sine[32:48]

    def make_kv(half):
        here = slice(half * ROWS, (half + 1) * ROWS)
        square = squares[here, :]
        scale = lax.rsqrt(jnp.sum(square, axis=1, keepdims=True) / width + epsilon)
        low = acc_ld[here, :] * scale
        low = low * lax.rsqrt(jnp.mean(low * low, axis=1, keepdims=True) + epsilon) * lgain_ref[0:1, :]
        expanded = jnp.dot(low.astype(jnp.bfloat16), up[...], preferred_element_type=jnp.float32)
        lane = lax.broadcasted_iota(jnp.int32, (ROWS, 128), 1)
        one, two = expanded[:, 0:128], expanded[:, 128:256]
        kv[half, 0:ROWS, :] = jnp.where(lane < HEAD, one, pltpu.roll(two, HEAD, 1)).astype(jnp.bfloat16)
        values = jnp.where(lane < HEAD, pltpu.roll(one, HEAD, 1), two)
        for k in range(2):
            kv[half, ROWS + 128 * k : ROWS + 128 * (k + 1), :] = jnp.transpose(
                values[128 * k : 128 * (k + 1)]
            ).astype(jnp.bfloat16)
        row_scale = lax.rsqrt(jnp.sum(jnp.transpose(square), axis=0, keepdims=True) / width + epsilon)
        shared = acc_slim[SLIM[2] : SLIM[3], here] * row_scale
        shared = turned(shared, ROPE // 2, slim_cos[:, here], slim_sin[:, here])
        shared = jnp.concatenate(shared, axis=0)
        groups = jnp.transpose(jnp.concatenate([shared[:, 0:128], shared[:, 128:256]] * 2, axis=0))
        packed = jnp.where(lane[0:64] < 64, groups[0:64], groups[64:128])
        kv[half, 2 * ROWS :, :] = packed.astype(jnp.bfloat16)
        send_kv(half)

    def make_q(half):
        here = slice(half * ROWS, (half + 1) * ROWS)
        total = jnp.sum(jnp.transpose(squares[here, :]), axis=0, keepdims=True)
        part = acc_slim[0 : SLIM[0], here] * lax.rsqrt(total / width + epsilon)
        wide = NOPE + ROPE
        pieces = [part[0:NOPE], part[wide : wide + NOPE]]
        for h in range(2):
            pieces += turned(
                part[wide * h + NOPE : wide * (h + 1)], ROPE // 2, slim_cos[:, here], slim_sin[:, here]
            )
        sharp = LOG2E * (NOPE + ROPE) ** (-0.5)
        q[:, here] = (jnp.concatenate(pieces, axis=0) * sharp).astype(jnp.bfloat16)
        send_q(half)

    to_side(0, True).wait_recv()
    onward(0, True).start()
    to_side(1, False).wait_recv()
    onward(0, False).start()
    to_side(3, True).start()
    to_side(2, False).start()
    over(0, 0).wait_recv()
    add(0, 0)
    to_side(1, True).wait_recv()
    over(1, 0).start()
    to_side(0, False).wait_recv()
    over(3, 0).start()
    over(1, 0).wait_recv()
    add(1, 0)
    over(3, 0).wait_recv()
    add(3, 0)
    to_side(2, True).wait_recv()
    onward(1, True).start()
    to_side(3, False).wait_recv()
    onward(1, False).start()
    onward(0, True).wait_recv()
    onward(0, False).wait_recv()
    over(2, 0).start()
    over(0, 1).wait_recv()
    add(0, 1)
    over(2, 0).wait_recv()
    add(2, 0)
    raise_ready()
    make_kv(0)
    make_q(0)
    to_side(3, True).wait_recv()
    over(1, 1).start()
    to_side(2, False).wait_recv()
    over(3, 1).start()
    over(1, 1).wait_recv()
    add(1, 1)
    over(3, 1).wait_recv()
    add(3, 1)
    onward(1, True).wait_recv()
    onward(1, False).wait_recv()
    over(2, 1).start()
    over(2, 1).wait_recv()
    add(2, 1)
    scale = lax.rsqrt(jnp.sum(squares[...], axis=1, keepdims=True) / width + epsilon)
    row_scale = lax.rsqrt(jnp.sum(jnp.transpose(squares[...]), axis=0, keepdims=True) / width + epsilon)
    mixed = acc_slim[0 : SLIM[2]] * row_scale
    keys = jnp.concatenate(turned(mixed[SLIM[0] : SLIM[1]], HEAD // 2, wide_cos, wide_sin), axis=0)
    values_t = mixed[SLIM[1] : SLIM[2]]
    wkv[...] = jnp.transpose(jnp.concatenate([keys, values_t], axis=0)).astype(jnp.bfloat16)
    send_w()
    make_kv(1)
    make_q(1)
    queries = jnp.transpose(acc_wq[...] * scale)
    pieces = []
    for h in range(2):
        pieces += turned(queries[HEAD * h : HEAD * (h + 1)], HEAD // 2, wide_cos, wide_sin)
    wq[...] = (jnp.concatenate(pieces, axis=0) * (LOG2E * HEAD ** (-0.5))).astype(jnp.bfloat16)

    sent = [to_side(quarter, way) for quarter in range(4) for way in (True, False)]
    sent += [onward(half, way) for half in range(2) for way in (True, False)]
    sent += [over(r, half) for r in range(X) for half in range(2)]
    return sent


def reduce(mixed, wl, ww, out_ref, pair_out, pair_in, passed, gone, kept, side_out, side_in, r_send, r_recv):
    tp = lax.axis_index("tp")
    x, core = tp // 2, tp % 2
    right = ((x + 1) % X) * 2 + core
    left = ((x + X - 1) % X) * 2 + core
    partner = 2 * x + 1 - core
    values = mixed[...]

    def projected(r, core_to):
        block = ((x + r) % X) * 2 + core_to
        cols = pl.ds(pl.multiple_of(block * COLS, COLS), COLS)
        weight = jnp.concatenate([wl[:, cols], ww[:, cols]], axis=0)
        return jnp.dot(values, weight, preferred_element_type=jnp.float32)

    def pair(r):
        return remote(pair_out.at[r], pair_in.at[r], r_send.at[r], r_recv.at[r], at_tp(partner))

    def far(half):
        return remote(
            gone.at[half], passed.at[half], r_send.at[4 + half], r_recv.at[4 + half], at_tp((right, left)[half])
        )

    def side(rightward, half):
        tag = 2 * (0 if rightward else 1) + half
        return remote(
            side_out.at[tag], side_in.at[tag], r_send.at[6 + tag], r_recv.at[6 + tag], at_tp(right if rightward else left)
        )

    def start_pair(r):
        pair_out[r] = projected(r, 1 - core).astype(jnp.bfloat16)
        pair(r).start()

    order = (2, 1, 3, 0)
    start_pair(2)
    own_next = projected(2, core)
    start_pair(1)
    for n, r in enumerate(order):
        own = own_next
        pair(r).wait_recv()
        total = own + pair_in[r].astype(jnp.float32)
        upper, lower = total[:ROWS], total[ROWS:]
        if r == 2:
            gone[0] = upper.astype(jnp.bfloat16)
            far(0).start()
            gone[1] = lower.astype(jnp.bfloat16)
            far(1).start()
        elif r == 1:
            side_out[1] = lower.astype(jnp.bfloat16)
            side(True, 1).start()
            kept[0] = upper
        elif r == 3:
            side_out[2] = upper.astype(jnp.bfloat16)
            side(False, 0).start()
            kept[1] = lower
        else:
            kept[2] = upper
            kept[3] = lower
        if n < 2:
            start_pair(order[n + 2])
        if n < 3:
            own_next = projected(order[n + 1], core)
    far(0).wait_recv()
    side_out[0] = (kept[0] + passed[0].astype(jnp.float32)).astype(jnp.bfloat16)
    side(True, 0).start()
    far(1).wait_recv()
    side_out[3] = (kept[1] + passed[1].astype(jnp.float32)).astype(jnp.bfloat16)
    side(False, 1).start()
    for half in (1, 0):
        side(True, half).wait_recv()
        side(False, half).wait_recv()
    for half in range(2):
        total = kept[2 + half] + side_in[half].astype(jnp.float32) + side_in[2 + half].astype(jnp.float32)
        out_ref[half * ROWS : (half + 1) * ROWS, :] = total.astype(jnp.bfloat16)
    sent = [pair(r) for r in range(X)] + [far(half) for half in range(2)]
    return sent + [side(way, half) for way in (True, False) for half in range(2)]


SLIM = (192, 256, 320, 352)


def layer_kernel(
    length_all,
    sink_ref,
    x_hbm,
    gain_hbm,
    lgain_hbm,
    near_hbm,
    far_hbm,
    lq_hbm,
    wk_hbm,
    wv_hbm,
    rd_hbm,
    ld_hbm,
    wq_hbm,
    up_hbm,
    ol_hbm,
    ow_hbm,
    result_ref,
    gain_ref,
    lgain_ref,
    near_ref,
    far_ref,
    w_slim,
    w_ld,
    w_wq,
    w_up,
    w_ol,
    w_ow,
    xs,
    squares,
    a_slim,
    a_ld,
    a_wq,
    q_ref,
    wkv_ref,
    wq_ref,
    out_ref,
    kvs,
    ropes,
    qraw,
    qpad,
    wkv,
    s0,
    s1,
    s2,
    s3,
    s4,
    s5,
    s6,
    s7,
    now_max,
    now_shrink,
    run_max,
    acc,
    o_out,
    o_in,
    pair_out,
    pair_in,
    passed,
    gone,
    kept,
    side_out,
    side_in,
    load_sem,
    x_send,
    x_recv,
    kv_send,
    kv_recv,
    q_send,
    q_recv,
    o_send,
    o_recv,
    w_send,
    w_recv,
    r_send,
    r_recv,
):
    sp = lax.axis_index("sp")
    z, y = sp // Y, sp % Y
    up = ((z + 1) % Z) * Y + y
    down = ((z + Z - 1) % Z) * Y + y
    right = z * Y + (y + 1) % Y
    left = z * Y + (y + Y - 1) % Y
    across = z * Y + (y + 2) % Y
    after = (sp + 1) % (Z * Y)
    before = (sp + Z * Y - 1) % (Z * Y)
    barrier = pltpu.get_barrier_semaphore()
    peers = [at_sp(peer) for peer in (up, down, right, left, across, after, before)]
    tp = lax.axis_index("tp")
    x, core = tp // 2, tp % 2
    peers += [at_tp((tp + 2) % (2 * X)), at_tp((tp + 2 * X - 2) % (2 * X)), at_tp(2 * x + 1 - core)]
    for peer in peers:
        pl.semaphore_signal(barrier, inc=1, device_id=peer, device_id_type=MESH)
    load_x = pltpu.make_async_copy(x_hbm, xs.at[core], load_sem.at[13])
    load_x.start()
    sources = (gain_hbm, lgain_hbm, near_hbm, far_hbm, lq_hbm, wk_hbm, wv_hbm, rd_hbm, ld_hbm, wq_hbm, up_hbm, ol_hbm, ow_hbm)
    ends = (0, *SLIM)
    targets = [gain_ref, lgain_ref, near_ref, far_ref]
    targets += [w_slim.at[pl.ds(a, b - a)] for a, b in zip(ends, SLIM)] + [w_ld, w_wq, w_up, w_ol, w_ow]
    loads = [
        pltpu.make_async_copy(source, target, load_sem.at[n])
        for n, (source, target) in enumerate(zip(sources, targets))
    ]
    load_x.wait()
    pl.semaphore_wait(barrier, len(peers))

    def copy(src, dst, send, recv, peer):
        return pltpu.make_async_remote_copy(
            src_ref=src,
            dst_ref=dst,
            send_sem=send,
            recv_sem=recv,
            device_id=at_sp(peer),
            device_id_type=MESH,
        )

    def kv_copy(step, half, upward):
        came = 0 if step == 1 else (2 * step - 3 if upward else 2 * step - 2)
        goes = 2 * step - 1 if upward else 2 * step
        slot = 2 * goes + half
        return copy(
            kvs.at[came, half], kvs.at[goes, half], kv_send.at[slot], kv_recv.at[slot], up if upward else down
        )

    def kv_last(half, upward):
        quarter = pl.ds(0 if upward else HALF // 2, HALF // 2)
        slot = 14 + 2 * half + (0 if upward else 1)
        return copy(
            kvs.at[5 if upward else 6, half, quarter],
            kvs.at[7, half, quarter],
            kv_send.at[slot],
            kv_recv.at[slot],
            up if upward else down,
        )

    def q_side(half, rightward):
        cols = pl.ds(half * ROWS, ROWS)
        tag = half + (0 if rightward else 2)
        return copy(
            q_ref.at[:, cols],
            qraw.at[1 if rightward else 2, :, cols],
            q_send.at[tag],
            q_recv.at[tag],
            right if rightward else left,
        )

    def q_onward(rightward):
        cols = pl.ds(0 if rightward else ROWS, ROWS)
        tag = 4 if rightward else 5
        return copy(
            qraw.at[1 if rightward else 2, :, cols],
            qraw.at[3, :, cols],
            q_send.at[tag],
            q_recv.at[tag],
            right if rightward else left,
        )

    w_after = copy(
        wkv_ref.at[pl.ds(BLK - WINDOW, WINDOW)], wkv.at[pl.ds(0, WINDOW)], w_send.at[0], w_recv.at[0], after
    )
    w_before = copy(
        wkv_ref.at[pl.ds(0, WINDOW)], wkv.at[pl.ds(BLK + WINDOW, WINDOW)], w_send.at[1], w_recv.at[1], before
    )

    def load_weights():
        for load in loads:
            load.start()
        run_max[...] = jnp.full(run_max.shape, -1e30, jnp.float32)
        acc[...] = jnp.zeros(acc.shape, jnp.float32)
        for load in loads[:-3]:
            load.wait()

    def send_kv(half):
        kv_copy(1, half, True).start()
        kv_copy(1, half, False).start()

    def send_q(half):
        q_side(half, True).start()
        q_side(half, False).start()

    def send_w():
        w_after.start()
        w_before.start()

    x_sent = project(
        gain_ref,
        lgain_ref,
        near_ref,
        far_ref,
        (w_slim, w_ld, w_wq),
        w_up,
        kvs.at[0],
        q_ref,
        wkv_ref,
        wq_ref,
        xs,
        squares,
        (a_slim, a_ld, a_wq),
        x_send,
        x_recv,
        load_weights,
        loads[-3].wait,
        send_kv,
        send_q,
        send_w,
    )

    tiles = (s0, s1, s2, s3, s4, s5, s6, s7)
    blank = jnp.zeros((NOPE, BLK), jnp.bfloat16)

    def set_queries(g, src):
        qpad[2 * g, 0:NOPE] = src[0:NOPE, :]
        qpad[2 * g, NOPE : 2 * NOPE] = blank
        qpad[2 * g + 1, 0:NOPE] = blank
        qpad[2 * g + 1, NOPE : 2 * NOPE] = src[NOPE : 2 * NOPE, :]
        for h in range(2):
            start = 2 * NOPE + h * ROPE
            qpad[2 * g + h, 2 * NOPE : 2 * NOPE + ROPE] = src[start : start + ROPE, :]
            qpad[2 * g + h, 2 * NOPE + ROPE :] = jnp.zeros((128 - ROPE, BLK), jnp.bfloat16)

    def set_ropes(p):
        for half in range(2):
            packed = kvs[p, half, 2 * ROWS :, :]
            wide = packed.astype(jnp.float32)
            start = half * ROWS
            ropes[p, start : start + 64] = packed
            for k, shift in enumerate((64, 96, 32)):
                turned_keys = pltpu.roll(wide, shift, 1).astype(jnp.bfloat16)
                ropes[p, start + 64 * (k + 1) : start + 64 * (k + 2)] = turned_keys

    def keys_of(p):
        keys = jnp.concatenate([kvs[p, 0, 0:ROWS, :], kvs[p, 1, 0:ROWS, :]], axis=0)
        return jnp.concatenate([keys, ropes[p]], axis=1)

    def scores_stage(unit, h, j, n):
        p, g = unit
        cols = slice(n * TILE, (n + 1) * TILE)
        scores = jnp.dot(keys_of(p), qpad[2 * g + h, :, cols], preferred_element_type=jnp.float32)
        tiles[4 * h + 2 * j + n][...] = scores
        before_max = run_max[2 * g + h, :, cols]
        highest = jnp.maximum(before_max, jnp.max(scores, axis=0, keepdims=True))
        now_shrink[2 * h + j, :, cols] = jnp.exp2(before_max - highest)
        now_max[2 * h + j, :, cols] = highest
        run_max[2 * g + h, :, cols] = highest

    def values_stage(unit, h, j, n):
        p, g = unit
        cols = slice(n * TILE, (n + 1) * TILE)
        weights = jnp.exp2(tiles[4 * h + 2 * j + n][...] - now_max[2 * h + j, :, cols]).astype(jnp.bfloat16)
        values = jnp.concatenate(
            [
                kvs[p, half, pl.ds(ROWS + 128 * k + HEAD * h, HEAD), :]
                for half in range(2)
                for k in range(2)
            ],
            axis=1,
        )
        values = jnp.concatenate([values, jnp.ones((16, BLK), jnp.bfloat16)], axis=0)
        mix = jnp.dot(values, weights, preferred_element_type=jnp.float32)
        acc[2 * g + h, :, cols] = acc[2 * g + h, :, cols] * now_shrink[2 * h + j, :, cols] + mix

    def finish(g, h):
        total = acc[2 * g + h]
        denominator = total[HEAD : HEAD + 1]
        return total[:HEAD] / denominator, run_max[2 * g + h] + jnp.log2(denominator)

    def o_copy(g):
        peer = (None, left, right, across)[g]
        return copy(o_out.at[g - 1], o_in.at[g - 1], o_send.at[g - 1], o_recv.at[g - 1], peer)

    def send_out(g):
        tails = []
        for h in range(2):
            out, level = finish(g, h)
            o_out[g - 1, HEAD * h : HEAD * (h + 1)] = out.astype(jnp.bfloat16)
            tails += [part.astype(jnp.float32) for part in split3(level)]
        tails.append(jnp.zeros((10, BLK), jnp.float32))
        o_out[g - 1, 2 * HEAD :] = jnp.concatenate(tails, axis=0).astype(jnp.bfloat16)
        o_copy(g).start()

    def unit(u):
        p, g = jnp.where(u < 3, 0, 1 + (u - 3) // 2), jnp.where(u < 3, u, 1 + (u - 3) % 2)
        p, g = jnp.where(u < 7, p, u - 7), jnp.where(u < 7, g, 3)
        p, g = jnp.where(u < 10, p, 3 + (u - 10) // 4), jnp.where(u < 10, g, (u - 10) % 4)
        p, g = jnp.where(u < 18, p, 5 + (u - 18) // 3), jnp.where(u < 18, g, 3 - (u - 18) % 3)
        p = jnp.where(u < 27, p, jnp.where(u < 29, u - 26, u - 24))
        g = jnp.where(u < 27, g, 0)
        return p, g

    set_queries(0, q_ref)
    set_ropes(0)
    for load in loads[-2:]:
        load.wait()
    wkv[WINDOW : WINDOW + BLK, :] = wkv_ref[...]
    def arrive(step, half):
        kv_copy(step, half, True).wait_recv()
        kv_copy(step, half, False).wait_recv()

    arrive(1, 0)
    kv_copy(2, 0, True).start()
    kv_copy(2, 0, False).start()
    w_after.wait_recv()
    w_before.wait_recv()
    window_part(wkv, wq_ref, sink_ref, out_ref, sp, length_all)

    q_side(0, True).wait_recv()
    q_onward(True).start()
    q_side(0, False).wait_recv()
    q_side(1, False).wait_recv()
    q_onward(False).start()
    q_side(1, True).wait_recv()
    set_queries(1, qraw.at[1])
    set_queries(2, qraw.at[2])
    parts = [(j, n) for j in range(2) for n in range(2)]
    for j, n in parts:
        scores_stage(unit(j), 0, j, n)

    def at0():
        arrive(1, 1)
        kv_copy(2, 1, True).start()
        kv_copy(2, 1, False).start()
        set_ropes(1)
        set_ropes(2)

    def at2():
        arrive(2, 0)
        kv_copy(3, 0, True).start()
        kv_copy(3, 0, False).start()
        q_onward(True).wait_recv()
        q_onward(False).wait_recv()
        set_queries(3, qraw.at[3])

    def at4():
        arrive(2, 1)
        kv_copy(3, 1, True).start()
        kv_copy(3, 1, False).start()
        set_ropes(3)
        set_ropes(4)

    def at6():
        arrive(3, 0)
        kv_last(0, True).start()
        kv_last(0, False).start()

    def at8():
        arrive(3, 1)
        kv_last(1, True).start()
        kv_last(1, False).start()
        set_ropes(5)
        set_ropes(6)

    def at11():
        for half in range(2):
            kv_last(half, True).wait_recv()
            kv_last(half, False).wait_recv()
        set_ropes(7)

    def at13():
        send_out(3)
        send_out(2)

    events = {0: at0, 2: at2, 4: at4, 6: at6, 8: at8, 11: at11, 13: at13, 14: lambda: send_out(1)}

    def advance(i, carry):
        for when, event in events.items():
            pl.when(i == when)(event)
        pair = [unit(2 * i), unit(2 * i + 1)]
        following = [unit(2 * i + 2), unit(2 * i + 3)]
        for j, n in parts:
            scores_stage(pair[j], 1, j, n)
            values_stage(pair[j], 0, j, n)
        for j, n in parts:
            scores_stage(following[j], 0, j, n)
            values_stage(pair[j], 1, j, n)
        return carry

    lax.fori_loop(0, PAIRS - 1, advance, 0)
    pair = [unit(2 * PAIRS - 2), unit(2 * PAIRS - 1)]
    for j, n in parts:
        scores_stage(pair[j], 1, j, n)
        values_stage(pair[j], 0, j, n)
    for j, n in parts:
        values_stage(pair[j], 1, j, n)

    own = [finish(0, h) for h in range(2)]
    for g in range(1, 4):
        o_copy(g).wait_recv()
    merged = []
    for h in range(2):
        outs, levels = [own[h][0]], [own[h][1]]
        for g in range(1, 4):
            block = o_in[g - 1].astype(jnp.float32)
            outs.append(block[HEAD * h : HEAD * (h + 1)])
            row = 2 * HEAD + 3 * h
            levels.append(block[row : row + 1] + block[row + 1 : row + 2] + block[row + 2 : row + 3])
        top = functools.reduce(jnp.maximum, levels)
        shares = [jnp.exp2(level - top) for level in levels]
        total = functools.reduce(jnp.add, shares)
        mixed = functools.reduce(jnp.add, [o * (s / total) for o, s in zip(outs, shares)])
        merged.append(mixed)
    out_ref[:, 0 : 2 * HEAD] = jnp.transpose(jnp.concatenate(merged, axis=0)).astype(jnp.bfloat16)

    r_sent = reduce(
        out_ref, w_ol, w_ow, result_ref, pair_out, pair_in, passed, gone, kept, side_out, side_in, r_send, r_recv
    )

    w_sends = [w_after, w_before, q_onward(True), q_onward(False)]
    w_sends += [q_side(half, way) for half in range(2) for way in (True, False)]
    for step in range(1, 4):
        for half in range(2):
            w_sends += [kv_copy(step, half, True), kv_copy(step, half, False)]
    w_sends += [kv_last(half, way) for half in range(2) for way in (True, False)]
    w_sends += [o_copy(g) for g in range(1, 4)]
    for sent in w_sends + x_sent + r_sent:
        sent.wait_send()


def tables():
    near, freqs = [], []
    for width in (HEAD, ROPE):
        half = width // 2
        freqs.append(10000.0 ** (-np.arange(half) / half))
    freqs = np.concatenate(freqs)
    angles = freqs[:, None] * np.arange(BLK)[None, :]
    near = np.stack([np.cos(angles), np.sin(angles)]).astype(np.float32)
    angles = freqs[:, None] * (BLK * np.arange(128))[None, :]
    far = np.stack([np.cos(angles), np.sin(angles)]).astype(np.float32)
    return near, far


def shards(
    inputs,
    norm_gain,
    latent_query,
    latent_down,
    rope_down,
    latent_gain,
    latent_up,
    window_query,
    window_key,
    window_value,
    sink_logit,
    out_latent,
    out_window,
):
    length_all = BLK * Z * Y
    near, far = tables()
    dma = pltpu.SemaphoreType.DMA
    bf16, f32 = jnp.bfloat16, jnp.float32
    in_vmem = pl.BlockSpec(memory_space=pltpu.VMEM)
    in_smem = pl.BlockSpec(memory_space=pltpu.SMEM)
    in_hbm = pl.BlockSpec(memory_space=pltpu.HBM)
    rows = norm_gain.shape[0]
    return pl.pallas_call(
        functools.partial(layer_kernel, length_all),
        out_shape=pltpu.VMEM((BLK, COLS), bf16),
        in_specs=[in_smem] + [in_hbm] * 14,
        out_specs=in_vmem,
        scratch_shapes=[
            pltpu.VMEM((1, rows), f32),
            pltpu.VMEM((1, latent_gain.shape[0]), f32),
            pltpu.VMEM(near.shape, f32),
            pltpu.VMEM(far.shape, f32),
            pltpu.VMEM((SLIM[3], rows), bf16),
            pltpu.VMEM(latent_down.shape, bf16),
            pltpu.VMEM(window_query.shape, bf16),
            pltpu.VMEM(latent_up.shape, bf16),
            pltpu.VMEM(out_latent.shape, bf16),
            pltpu.VMEM(out_window.shape, bf16),
            pltpu.VMEM((2 * X, BLK, COLS), bf16),
            pltpu.VMEM((BLK, 128), f32),
            pltpu.VMEM((SLIM[3], BLK), f32),
            pltpu.VMEM((BLK, latent_down.shape[1]), f32),
            pltpu.VMEM((BLK, window_query.shape[1]), f32),
            pltpu.VMEM((2 * (NOPE + ROPE), BLK), bf16),
            pltpu.VMEM((BLK, 2 * HEAD), bf16),
            pltpu.VMEM((2 * HEAD, BLK), bf16),
            pltpu.VMEM((BLK, 4 * HEAD), bf16),
            pltpu.VMEM((Z, 2, HALF, 128), bf16),
            pltpu.VMEM((Z, BLK, 128), bf16),
            pltpu.VMEM((Y, 2 * (NOPE + ROPE), BLK), bf16),
            pltpu.VMEM((2 * Y, 256, BLK), bf16),
            pltpu.VMEM((BLK + 2 * WINDOW, 128), bf16),
            *[pltpu.VMEM((BLK, TILE), f32)] * 8,
            pltpu.VMEM((4, 1, BLK), f32),
            pltpu.VMEM((4, 1, BLK), f32),
            pltpu.VMEM((2 * Y, 1, BLK), f32),
            pltpu.VMEM((2 * Y, HEAD + 16, BLK), f32),
            pltpu.VMEM((Y - 1, O_ROWS, BLK), bf16),
            pltpu.VMEM((Y - 1, O_ROWS, BLK), bf16),
            pltpu.VMEM((X, BLK, COLS), bf16),
            pltpu.VMEM((X, BLK, COLS), bf16),
            pltpu.VMEM((2, ROWS, COLS), bf16),
            pltpu.VMEM((2, ROWS, COLS), bf16),
            pltpu.VMEM((4, ROWS, COLS), f32),
            pltpu.VMEM((4, ROWS, COLS), bf16),
            pltpu.VMEM((4, ROWS, COLS), bf16),
            dma((14,)),
            dma((20,)),
            dma((20,)),
            dma((18,)),
            dma((18,)),
            dma((6,)),
            dma((6,)),
            dma((3,)),
            dma((3,)),
            dma((2,)),
            dma((2,)),
            dma((10,)),
            dma((10,)),
        ],
        compiler_params=pltpu.CompilerParams(
            collective_id=1, has_side_effects=True, vmem_limit_bytes=VMEM_LIMIT
        ),
        name="layer",
    )(
        sink_logit,
        inputs,
        norm_gain[None, :],
        latent_gain[None, :],
        near,
        far,
        latent_query.T,
        window_key.T,
        window_value.T,
        rope_down.T,
        latent_down,
        window_query,
        latent_up,
        out_latent,
        out_window,
    )


def solution(mesh):
    in_specs = (
        P("sp", "tp"),
        P(),
        P(None, "tp"),
        P(),
        P(),
        P(),
        P(None, "tp"),
        P(None, "tp"),
        P(None, "tp"),
        P(None, "tp"),
        P("tp"),
        P("tp", None),
        P("tp", None),
    )
    out_specs = P("sp", "tp")
    return jax.shard_map(shards, mesh=mesh, in_specs=in_specs, out_specs=out_specs, check_vma=False)
```

```python
import functools

import jax
import jax.numpy as jnp
import numpy as np
from jax import lax
from jax.experimental import pallas as pl
from jax.experimental.pallas import tpu as pltpu
from jax.sharding import PartitionSpec as P

NOPE = 64
ROPE = 32
HEAD = 64
WINDOW = 128
LOG2E = 1.4426950408889634

MESH = pl.DeviceIdType.MESH
VMEM_LIMIT = 60 * 2**20
Z, Y, X = 8, 4, 4
BLK = 512
HALF = BLK // 2 + BLK // 2 + BLK // 8
O_ROWS = 2 * HEAD + 16
COLS = 256
ROWS = BLK // 2
QUARTER = BLK // 4
TILE = 256
PAIRS = Y * Z // 2


epsilon = 1e-06


def at_sp(index):
    return {"sp": index}


def split3(value):
    high = value.astype(jnp.bfloat16)
    rest = value - high.astype(jnp.float32)
    middle = rest.astype(jnp.bfloat16)
    low = (rest - middle.astype(jnp.float32)).astype(jnp.bfloat16)
    return high, middle, low


def window_part(wkv, wq_ref, sink_ref, out_ref, sp, length_all):
    values_t = jnp.transpose(wkv[...].astype(jnp.float32))[HEAD:, :].astype(jnp.bfloat16)
    lane = lax.broadcasted_iota(jnp.int32, (1, 2 * WINDOW), 1)
    sinks = jnp.where(lane < WINDOW, sink_ref[0], sink_ref[1]) * LOG2E
    rows = lax.broadcasted_iota(jnp.int32, (3 * WINDOW, 2 * WINDOW), 0)
    cols = lax.broadcasted_iota(jnp.int32, (3 * WINDOW, 2 * WINDOW), 1)
    gap = rows - cols % WINDOW
    near = (gap >= 0) & (gap <= 2 * WINDOW)
    blank = jnp.zeros((HEAD, WINDOW), jnp.bfloat16)
    for n in range(BLK // WINDOW):
        here = slice(n * WINDOW, (n + 1) * WINDOW)
        keys = wkv[n * WINDOW : (n + 3) * WINDOW, :]
        queries = jnp.concatenate(
            [
                jnp.concatenate([wq_ref[0:HEAD, here], blank], axis=0),
                jnp.concatenate([wq_ref[HEAD : 2 * HEAD, here], blank], axis=0),
            ],
            axis=1,
        )
        scores = jnp.dot(keys, queries, preferred_element_type=jnp.float32)
        place = rows + (sp * BLK + (n - 1) * WINDOW)
        allowed = near & (place >= 0) & (place < length_all)
        scores = jnp.where(allowed, scores, -jnp.inf)
        highest = jnp.maximum(jnp.max(scores, axis=0, keepdims=True), sinks)
        weights = jnp.exp2(scores - highest)
        denominators = jnp.sum(weights, axis=0, keepdims=True) + jnp.exp2(sinks - highest)
        mix = jnp.dot(
            values_t[:, n * WINDOW : (n + 3) * WINDOW],
            weights.astype(jnp.bfloat16),
            preferred_element_type=jnp.float32,
        )
        mix = mix / denominators
        both = jnp.concatenate([mix[:, :WINDOW], mix[:, WINDOW:]], axis=0)
        out_ref[here, 2 * HEAD :] = jnp.transpose(both).astype(jnp.bfloat16)


def at_tp(index):
    return {"tp": index}


def remote(src, dst, send, recv, device):
    return pltpu.make_async_remote_copy(
        src_ref=src, dst_ref=dst, send_sem=send, recv_sem=recv, device_id=device, device_id_type=MESH
    )


def turned(rows, half, cosine, sine):
    first, second = rows[:half], rows[half:]
    return [first * cosine - second * sine, second * cosine + first * sine]


def project(
    gain_ref, lgain_ref, near_ref, far_ref, weights, up, kv, q, wkv, wq, xs, squares, accs, x_send, x_recv, ready, raise_ready, send_kv, send_q, send_w
):
    tp = lax.axis_index("tp")
    x, core = tp // 2, tp % 2
    right = ((x + 1) % X) * 2 + core
    left = ((x + X - 1) % X) * 2 + core
    partner = 2 * x + 1 - core

    def rows_of(ref, start, size):
        return ref.at[pl.ds(start, size)]

    mine = [2 * r + core for r in range(X)]

    def to_side(quarter, rightward):
        slot = mine[1] if rightward else mine[3]
        tag = quarter + (0 if rightward else 4)
        return remote(
            rows_of(xs.at[core], quarter * QUARTER, QUARTER),
            rows_of(xs.at[slot], quarter * QUARTER, QUARTER),
            x_send.at[tag],
            x_recv.at[tag],
            at_tp(right if rightward else left),
        )

    def onward(half, rightward):
        start = half * ROWS + (0 if rightward else QUARTER)
        tag = 8 + 2 * half + (0 if rightward else 1)
        return remote(
            rows_of(xs.at[mine[1] if rightward else mine[3]], start, QUARTER),
            rows_of(xs.at[mine[2]], start, QUARTER),
            x_send.at[tag],
            x_recv.at[tag],
            at_tp(right if rightward else left),
        )

    def over(r, half):
        tag = 12 + 2 * r + half
        slot = rows_of(xs.at[mine[r]], half * ROWS, ROWS)
        return remote(slot, slot, x_send.at[tag], x_recv.at[tag], at_tp(partner))

    for quarter in (0, 1, 2):
        to_side(quarter, True).start()
        to_side((1, 0, 3)[quarter], False).start()
    over(0, 0).start()
    over(0, 1).start()
    ready()

    def add(r, half):
        chip = (x + (0, X - 1, 2, 1)[r]) % X
        here = slice(half * ROWS, (half + 1) * ROWS)
        values = jnp.concatenate([xs[2 * r, here], xs[2 * r + 1, here]], axis=1).astype(jnp.float32)
        square = values * values
        square = square[:, 0:128] + square[:, 128:256] + square[:, 256:384] + square[:, 384:512]
        rows = pl.ds(pl.multiple_of(chip * 2 * COLS, 2 * COLS), 2 * COLS)
        scaled = (values * gain_ref[:, rows]).astype(jnp.bfloat16)
        slim = lax.dot_general(
            weights[0][:, rows], scaled, (((1,), (1,)), ((), ())), preferred_element_type=jnp.float32
        )
        wide = [jnp.dot(scaled, weight[rows, :], preferred_element_type=jnp.float32) for weight in weights[1:]]
        if r == 0:
            squares[here, :] = square
            accs[0][:, here] = slim
            for product, acc in zip(wide, accs[1:]):
                acc[here, :] = product
        else:
            squares[here, :] += square
            accs[0][:, here] += slim
            for product, acc in zip(wide, accs[1:]):
                acc[here, :] += product

    width = 2 * COLS * X
    acc_slim, acc_ld, acc_wq = accs
    turn = far_ref[...]
    here = lax.broadcasted_iota(jnp.int32, turn.shape, 2) == lax.axis_index("sp")
    turn = jnp.sum(jnp.where(here, turn, 0.0), axis=2, keepdims=True)
    far_cos, far_sin = turn[0], turn[1]
    near_cos, near_sin = near_ref[0], near_ref[1]
    cosine = far_cos * near_cos - far_sin * near_sin
    sine = far_sin * near_cos + far_cos * near_sin
    wide_cos, wide_sin = cosine[0:32], sine[0:32]
    slim_cos, slim_sin = cosine[32:48], sine[32:48]

    def make_kv(half):
        here = slice(half * ROWS, (half + 1) * ROWS)
        square = squares[here, :]
        scale = lax.rsqrt(jnp.sum(square, axis=1, keepdims=True) / width + epsilon)
        low = acc_ld[here, :] * scale
        low = low * lax.rsqrt(jnp.mean(low * low, axis=1, keepdims=True) + epsilon) * lgain_ref[0:1, :]
        expanded = jnp.dot(low.astype(jnp.bfloat16), up[...], preferred_element_type=jnp.float32)
        lane = lax.broadcasted_iota(jnp.int32, (ROWS, 128), 1)
        one, two = expanded[:, 0:128], expanded[:, 128:256]
        kv[half, 0:ROWS, :] = jnp.where(lane < HEAD, one, pltpu.roll(two, HEAD, 1)).astype(jnp.bfloat16)
        values = jnp.where(lane < HEAD, pltpu.roll(one, HEAD, 1), two)
        for k in range(2):
            kv[half, ROWS + 128 * k : ROWS + 128 * (k + 1), :] = jnp.transpose(
                values[128 * k : 128 * (k + 1)]
            ).astype(jnp.bfloat16)
        row_scale = lax.rsqrt(jnp.sum(jnp.transpose(square), axis=0, keepdims=True) / width + epsilon)
        shared = acc_slim[SLIM[2] : SLIM[3], here] * row_scale
        shared = turned(shared, ROPE // 2, slim_cos[:, here], slim_sin[:, here])
        shared = jnp.concatenate(shared, axis=0)
        groups = jnp.transpose(jnp.concatenate([shared[:, 0:128], shared[:, 128:256]] * 2, axis=0))
        packed = jnp.where(lane[0:64] < 64, groups[0:64], groups[64:128])
        kv[half, 2 * ROWS :, :] = packed.astype(jnp.bfloat16)
        send_kv(half)

    def make_q(half):
        here = slice(half * ROWS, (half + 1) * ROWS)
        total = jnp.sum(jnp.transpose(squares[here, :]), axis=0, keepdims=True)
        part = acc_slim[0 : SLIM[0], here] * lax.rsqrt(total / width + epsilon)
        wide = NOPE + ROPE
        pieces = [part[0:NOPE], part[wide : wide + NOPE]]
        for h in range(2):
            pieces += turned(
                part[wide * h + NOPE : wide * (h + 1)], ROPE // 2, slim_cos[:, here], slim_sin[:, here]
            )
        sharp = LOG2E * (NOPE + ROPE) ** (-0.5)
        q[:, here] = (jnp.concatenate(pieces, axis=0) * sharp).astype(jnp.bfloat16)
        send_q(half)

    to_side(0, True).wait_recv()
    onward(0, True).start()
    to_side(1, False).wait_recv()
    onward(0, False).start()
    to_side(3, True).start()
    to_side(2, False).start()
    over(0, 0).wait_recv()
    add(0, 0)
    to_side(1, True).wait_recv()
    over(1, 0).start()
    to_side(0, False).wait_recv()
    over(3, 0).start()
    over(1, 0).wait_recv()
    add(1, 0)
    over(3, 0).wait_recv()
    add(3, 0)
    to_side(2, True).wait_recv()
    onward(1, True).start()
    to_side(3, False).wait_recv()
    onward(1, False).start()
    onward(0, True).wait_recv()
    onward(0, False).wait_recv()
    over(2, 0).start()
    over(0, 1).wait_recv()
    add(0, 1)
    over(2, 0).wait_recv()
    add(2, 0)
    raise_ready()
    make_kv(0)
    make_q(0)
    to_side(3, True).wait_recv()
    over(1, 1).start()
    to_side(2, False).wait_recv()
    over(3, 1).start()
    over(1, 1).wait_recv()
    add(1, 1)
    over(3, 1).wait_recv()
    add(3, 1)
    onward(1, True).wait_recv()
    onward(1, False).wait_recv()
    over(2, 1).start()
    over(2, 1).wait_recv()
    add(2, 1)
    scale = lax.rsqrt(jnp.sum(squares[...], axis=1, keepdims=True) / width + epsilon)
    row_scale = lax.rsqrt(jnp.sum(jnp.transpose(squares[...]), axis=0, keepdims=True) / width + epsilon)
    mixed = acc_slim[0 : SLIM[2]] * row_scale
    keys = jnp.concatenate(turned(mixed[SLIM[0] : SLIM[1]], HEAD // 2, wide_cos, wide_sin), axis=0)
    values_t = mixed[SLIM[1] : SLIM[2]]
    wkv[...] = jnp.transpose(jnp.concatenate([keys, values_t], axis=0)).astype(jnp.bfloat16)
    send_w()
    make_kv(1)
    make_q(1)
    queries = jnp.transpose(acc_wq[...] * scale)
    pieces = []
    for h in range(2):
        pieces += turned(queries[HEAD * h : HEAD * (h + 1)], HEAD // 2, wide_cos, wide_sin)
    wq[...] = (jnp.concatenate(pieces, axis=0) * (LOG2E * HEAD ** (-0.5))).astype(jnp.bfloat16)

    sent = [to_side(quarter, way) for quarter in range(4) for way in (True, False)]
    sent += [onward(half, way) for half in range(2) for way in (True, False)]
    sent += [over(r, half) for r in range(X) for half in range(2)]
    return sent


def reduce(mixed, wl, ww, out_ref, pair_out, pair_in, passed, gone, kept, side_out, side_in, r_send, r_recv):
    tp = lax.axis_index("tp")
    x, core = tp // 2, tp % 2
    right = ((x + 1) % X) * 2 + core
    left = ((x + X - 1) % X) * 2 + core
    partner = 2 * x + 1 - core
    values = mixed[...]

    def projected(r, core_to, half):
        block = ((x + r) % X) * 2 + core_to
        cols = pl.ds(pl.multiple_of(block * COLS, COLS), COLS)
        weight = jnp.concatenate([wl[:, cols], ww[:, cols]], axis=0)
        return jnp.dot(values[half * ROWS : (half + 1) * ROWS], weight, preferred_element_type=jnp.float32)

    def pair(r, half):
        rows = pl.ds(half * ROWS, ROWS)
        tag = 6 + 2 * r + half + 4
        return remote(
            pair_out.at[r, rows], pair_in.at[r, rows], r_send.at[tag], r_recv.at[tag], at_tp(partner)
        )

    def far(half):
        return remote(
            gone.at[half], passed.at[half], r_send.at[4 + half], r_recv.at[4 + half], at_tp((right, left)[half])
        )

    def side(rightward, half):
        tag = 2 * (0 if rightward else 1) + half
        return remote(
            side_out.at[tag], side_in.at[tag], r_send.at[6 + tag], r_recv.at[6 + tag], at_tp(right if rightward else left)
        )

    def start_pair(r):
        for half in range(2):
            rows = slice(half * ROWS, (half + 1) * ROWS)
            pair_out[r, rows] = projected(r, 1 - core, half).astype(jnp.bfloat16)
            pair(r, half).start()

    def total_of(r, half, own):
        pair(r, half).wait_recv()
        return own + pair_in[r, half * ROWS : (half + 1) * ROWS].astype(jnp.float32)

    order = (2, 1, 3, 0)
    start_pair(2)
    own_next = [projected(2, core, half) for half in range(2)]
    start_pair(1)
    for n, r in enumerate(order):
        own = own_next
        if r == 2:
            for half in range(2):
                gone[half] = total_of(r, half, own[half]).astype(jnp.bfloat16)
                far(half).start()
        else:
            upper, lower = total_of(r, 0, own[0]), total_of(r, 1, own[1])
        if r == 2:
            pass
        elif r == 1:
            side_out[1] = lower.astype(jnp.bfloat16)
            side(True, 1).start()
            kept[0] = upper
        elif r == 3:
            side_out[2] = upper.astype(jnp.bfloat16)
            side(False, 0).start()
            kept[1] = lower
        else:
            kept[2] = upper
            kept[3] = lower
        if n < 2:
            start_pair(order[n + 2])
        if n < 3:
            own_next = [projected(order[n + 1], core, half) for half in range(2)]
    far(0).wait_recv()
    side_out[0] = (kept[0] + passed[0].astype(jnp.float32)).astype(jnp.bfloat16)
    side(True, 0).start()
    far(1).wait_recv()
    side_out[3] = (kept[1] + passed[1].astype(jnp.float32)).astype(jnp.bfloat16)
    side(False, 1).start()
    for half in (1, 0):
        side(True, half).wait_recv()
        side(False, half).wait_recv()
    for half in range(2):
        total = kept[2 + half] + side_in[half].astype(jnp.float32) + side_in[2 + half].astype(jnp.float32)
        out_ref[half * ROWS : (half + 1) * ROWS, :] = total.astype(jnp.bfloat16)
    sent = [pair(r, half) for r in range(X) for half in range(2)] + [far(half) for half in range(2)]
    return sent + [side(way, half) for way in (True, False) for half in range(2)]


SLIM = (192, 256, 320, 352)


def layer_kernel(
    length_all,
    sink_ref,
    x_hbm,
    gain_hbm,
    lgain_hbm,
    near_hbm,
    far_hbm,
    lq_hbm,
    wk_hbm,
    wv_hbm,
    rd_hbm,
    ld_hbm,
    wq_hbm,
    up_hbm,
    ol_hbm,
    ow_hbm,
    result_ref,
    gain_ref,
    lgain_ref,
    near_ref,
    far_ref,
    w_slim,
    w_ld,
    w_wq,
    w_up,
    w_ol,
    w_ow,
    xs,
    squares,
    a_slim,
    a_ld,
    a_wq,
    q_ref,
    wkv_ref,
    wq_ref,
    out_ref,
    kvs,
    ropes,
    qraw,
    qpad,
    wkv,
    s0,
    s1,
    s2,
    s3,
    s4,
    s5,
    s6,
    s7,
    now_max,
    now_shrink,
    run_max,
    acc,
    o_out,
    o_in,
    pair_out,
    pair_in,
    passed,
    gone,
    kept,
    side_out,
    side_in,
    load_sem,
    x_send,
    x_recv,
    kv_send,
    kv_recv,
    q_send,
    q_recv,
    o_send,
    o_recv,
    w_send,
    w_recv,
    r_send,
    r_recv,
):
    sp = lax.axis_index("sp")
    z, y = sp // Y, sp % Y
    up = ((z + 1) % Z) * Y + y
    down = ((z + Z - 1) % Z) * Y + y
    right = z * Y + (y + 1) % Y
    left = z * Y + (y + Y - 1) % Y
    across = z * Y + (y + 2) % Y
    after = (sp + 1) % (Z * Y)
    before = (sp + Z * Y - 1) % (Z * Y)
    barrier = pltpu.get_barrier_semaphore()
    peers = [at_sp(peer) for peer in (up, down, right, left, across, after, before)]
    tp = lax.axis_index("tp")
    x, core = tp // 2, tp % 2
    peers += [at_tp((tp + 2) % (2 * X)), at_tp((tp + 2 * X - 2) % (2 * X)), at_tp(2 * x + 1 - core)]
    for peer in peers:
        pl.semaphore_signal(barrier, inc=1, device_id=peer, device_id_type=MESH)
    load_x = pltpu.make_async_copy(x_hbm, xs.at[core], load_sem.at[13])
    load_x.start()
    sources = (gain_hbm, lgain_hbm, near_hbm, far_hbm, lq_hbm, wk_hbm, wv_hbm, rd_hbm, ld_hbm, wq_hbm, up_hbm, ol_hbm, ow_hbm)
    ends = (0, *SLIM)
    targets = [gain_ref, lgain_ref, near_ref, far_ref]
    targets += [w_slim.at[pl.ds(a, b - a)] for a, b in zip(ends, SLIM)] + [w_ld, w_wq, w_up, w_ol, w_ow]
    loads = [
        pltpu.make_async_copy(source, target, load_sem.at[n])
        for n, (source, target) in enumerate(zip(sources, targets))
    ]
    load_x.wait()
    pl.semaphore_wait(barrier, len(peers))

    def copy(src, dst, send, recv, peer):
        return pltpu.make_async_remote_copy(
            src_ref=src,
            dst_ref=dst,
            send_sem=send,
            recv_sem=recv,
            device_id=at_sp(peer),
            device_id_type=MESH,
        )

    def kv_copy(step, half, upward):
        came = 0 if step == 1 else (2 * step - 3 if upward else 2 * step - 2)
        goes = 2 * step - 1 if upward else 2 * step
        slot = 2 * goes + half
        return copy(
            kvs.at[came, half], kvs.at[goes, half], kv_send.at[slot], kv_recv.at[slot], up if upward else down
        )

    def kv_last(half, upward):
        quarter = pl.ds(0 if upward else HALF // 2, HALF // 2)
        slot = 14 + 2 * half + (0 if upward else 1)
        return copy(
            kvs.at[5 if upward else 6, half, quarter],
            kvs.at[7, half, quarter],
            kv_send.at[slot],
            kv_recv.at[slot],
            up if upward else down,
        )

    def q_side(half, rightward):
        cols = pl.ds(half * ROWS, ROWS)
        tag = half + (0 if rightward else 2)
        return copy(
            q_ref.at[:, cols],
            qraw.at[1 if rightward else 2, :, cols],
            q_send.at[tag],
            q_recv.at[tag],
            right if rightward else left,
        )

    def q_onward(rightward):
        cols = pl.ds(0 if rightward else ROWS, ROWS)
        tag = 4 if rightward else 5
        return copy(
            qraw.at[1 if rightward else 2, :, cols],
            qraw.at[3, :, cols],
            q_send.at[tag],
            q_recv.at[tag],
            right if rightward else left,
        )

    w_after = copy(
        wkv_ref.at[pl.ds(BLK - WINDOW, WINDOW)], wkv.at[pl.ds(0, WINDOW)], w_send.at[0], w_recv.at[0], after
    )
    w_before = copy(
        wkv_ref.at[pl.ds(0, WINDOW)], wkv.at[pl.ds(BLK + WINDOW, WINDOW)], w_send.at[1], w_recv.at[1], before
    )

    def load_weights():
        for load in loads:
            load.start()
        run_max[...] = jnp.full(run_max.shape, -1e30, jnp.float32)
        acc[...] = jnp.zeros(acc.shape, jnp.float32)
        for load in loads[:-3]:
            load.wait()

    def send_kv(half):
        kv_copy(1, half, True).start()
        kv_copy(1, half, False).start()

    def send_q(half):
        q_side(half, True).start()
        q_side(half, False).start()

    def send_w():
        w_after.start()
        w_before.start()

    x_sent = project(
        gain_ref,
        lgain_ref,
        near_ref,
        far_ref,
        (w_slim, w_ld, w_wq),
        w_up,
        kvs.at[0],
        q_ref,
        wkv_ref,
        wq_ref,
        xs,
        squares,
        (a_slim, a_ld, a_wq),
        x_send,
        x_recv,
        load_weights,
        loads[-3].wait,
        send_kv,
        send_q,
        send_w,
    )

    tiles = (s0, s1, s2, s3, s4, s5, s6, s7)
    blank = jnp.zeros((NOPE, BLK), jnp.bfloat16)

    def set_queries(g, src):
        qpad[2 * g, 0:NOPE] = src[0:NOPE, :]
        qpad[2 * g, NOPE : 2 * NOPE] = blank
        qpad[2 * g + 1, 0:NOPE] = blank
        qpad[2 * g + 1, NOPE : 2 * NOPE] = src[NOPE : 2 * NOPE, :]
        for h in range(2):
            start = 2 * NOPE + h * ROPE
            qpad[2 * g + h, 2 * NOPE : 2 * NOPE + ROPE] = src[start : start + ROPE, :]
            qpad[2 * g + h, 2 * NOPE + ROPE :] = jnp.zeros((128 - ROPE, BLK), jnp.bfloat16)

    def set_ropes(p):
        for half in range(2):
            packed = kvs[p, half, 2 * ROWS :, :]
            wide = packed.astype(jnp.float32)
            start = half * ROWS
            ropes[p, start : start + 64] = packed
            for k, shift in enumerate((64, 96, 32)):
                turned_keys = pltpu.roll(wide, shift, 1).astype(jnp.bfloat16)
                ropes[p, start + 64 * (k + 1) : start + 64 * (k + 2)] = turned_keys

    def keys_of(p):
        keys = jnp.concatenate([kvs[p, 0, 0:ROWS, :], kvs[p, 1, 0:ROWS, :]], axis=0)
        return jnp.concatenate([keys, ropes[p]], axis=1)

    def scores_stage(unit, h, j, n):
        p, g = unit
        cols = slice(n * TILE, (n + 1) * TILE)
        scores = jnp.dot(keys_of(p), qpad[2 * g + h, :, cols], preferred_element_type=jnp.float32)
        tiles[4 * h + 2 * j + n][...] = scores
        before_max = run_max[2 * g + h, :, cols]
        highest = jnp.maximum(before_max, jnp.max(scores, axis=0, keepdims=True))
        now_shrink[2 * h + j, :, cols] = jnp.exp2(before_max - highest)
        now_max[2 * h + j, :, cols] = highest
        run_max[2 * g + h, :, cols] = highest

    def values_stage(unit, h, j, n):
        p, g = unit
        cols = slice(n * TILE, (n + 1) * TILE)
        weights = jnp.exp2(tiles[4 * h + 2 * j + n][...] - now_max[2 * h + j, :, cols]).astype(jnp.bfloat16)
        values = jnp.concatenate(
            [
                kvs[p, half, pl.ds(ROWS + 128 * k + HEAD * h, HEAD), :]
                for half in range(2)
                for k in range(2)
            ],
            axis=1,
        )
        values = jnp.concatenate([values, jnp.ones((16, BLK), jnp.bfloat16)], axis=0)
        mix = jnp.dot(values, weights, preferred_element_type=jnp.float32)
        acc[2 * g + h, :, cols] = acc[2 * g + h, :, cols] * now_shrink[2 * h + j, :, cols] + mix

    def finish(g, h):
        total = acc[2 * g + h]
        denominator = total[HEAD : HEAD + 1]
        return total[:HEAD] / denominator, run_max[2 * g + h] + jnp.log2(denominator)

    def o_copy(g):
        peer = (None, left, right, across)[g]
        return copy(o_out.at[g - 1], o_in.at[g - 1], o_send.at[g - 1], o_recv.at[g - 1], peer)

    def send_out(g):
        tails = []
        for h in range(2):
            out, level = finish(g, h)
            o_out[g - 1, HEAD * h : HEAD * (h + 1)] = out.astype(jnp.bfloat16)
            tails += [part.astype(jnp.float32) for part in split3(level)]
        tails.append(jnp.zeros((10, BLK), jnp.float32))
        o_out[g - 1, 2 * HEAD :] = jnp.concatenate(tails, axis=0).astype(jnp.bfloat16)
        o_copy(g).start()

    def unit(u):
        p, g = jnp.where(u < 3, 0, 1 + (u - 3) // 2), jnp.where(u < 3, u, 1 + (u - 3) % 2)
        p, g = jnp.where(u < 7, p, u - 7), jnp.where(u < 7, g, 3)
        p, g = jnp.where(u < 10, p, 3 + (u - 10) // 4), jnp.where(u < 10, g, (u - 10) % 4)
        p, g = jnp.where(u < 18, p, 5 + (u - 18) // 3), jnp.where(u < 18, g, 3 - (u - 18) % 3)
        p = jnp.where(u < 27, p, jnp.where(u < 29, u - 26, u - 24))
        g = jnp.where(u < 27, g, 0)
        return p, g

    set_queries(0, q_ref)
    set_ropes(0)
    for load in loads[-2:]:
        load.wait()
    wkv[WINDOW : WINDOW + BLK, :] = wkv_ref[...]
    def arrive(step, half):
        kv_copy(step, half, True).wait_recv()
        kv_copy(step, half, False).wait_recv()

    arrive(1, 0)
    kv_copy(2, 0, True).start()
    kv_copy(2, 0, False).start()
    w_after.wait_recv()
    w_before.wait_recv()
    window_part(wkv, wq_ref, sink_ref, out_ref, sp, length_all)

    q_side(0, True).wait_recv()
    q_onward(True).start()
    q_side(0, False).wait_recv()
    q_side(1, False).wait_recv()
    q_onward(False).start()
    q_side(1, True).wait_recv()
    set_queries(1, qraw.at[1])
    set_queries(2, qraw.at[2])
    parts = [(j, n) for j in range(2) for n in range(2)]
    for j, n in parts:
        scores_stage(unit(j), 0, j, n)

    def at0():
        arrive(1, 1)
        kv_copy(2, 1, True).start()
        kv_copy(2, 1, False).start()
        set_ropes(1)
        set_ropes(2)

    def at2():
        arrive(2, 0)
        kv_copy(3, 0, True).start()
        kv_copy(3, 0, False).start()
        q_onward(True).wait_recv()
        q_onward(False).wait_recv()
        set_queries(3, qraw.at[3])

    def at4():
        arrive(2, 1)
        kv_copy(3, 1, True).start()
        kv_copy(3, 1, False).start()
        set_ropes(3)
        set_ropes(4)

    def at6():
        arrive(3, 0)
        kv_last(0, True).start()
        kv_last(0, False).start()

    def at8():
        arrive(3, 1)
        kv_last(1, True).start()
        kv_last(1, False).start()
        set_ropes(5)
        set_ropes(6)

    def at11():
        for half in range(2):
            kv_last(half, True).wait_recv()
            kv_last(half, False).wait_recv()
        set_ropes(7)

    def at13():
        send_out(3)
        send_out(2)

    events = {0: at0, 2: at2, 4: at4, 6: at6, 8: at8, 11: at11, 13: at13, 14: lambda: send_out(1)}

    def advance(i, carry):
        for when, event in events.items():
            pl.when(i == when)(event)
        pair = [unit(2 * i), unit(2 * i + 1)]
        following = [unit(2 * i + 2), unit(2 * i + 3)]
        for j, n in parts:
            scores_stage(pair[j], 1, j, n)
            values_stage(pair[j], 0, j, n)
        for j, n in parts:
            scores_stage(following[j], 0, j, n)
            values_stage(pair[j], 1, j, n)
        return carry

    lax.fori_loop(0, PAIRS - 1, advance, 0)
    pair = [unit(2 * PAIRS - 2), unit(2 * PAIRS - 1)]
    for j, n in parts:
        scores_stage(pair[j], 1, j, n)
        values_stage(pair[j], 0, j, n)
    for j, n in parts:
        values_stage(pair[j], 1, j, n)

    own = [finish(0, h) for h in range(2)]
    for g in range(1, 4):
        o_copy(g).wait_recv()
    merged = []
    for h in range(2):
        outs, levels = [own[h][0]], [own[h][1]]
        for g in range(1, 4):
            block = o_in[g - 1].astype(jnp.float32)
            outs.append(block[HEAD * h : HEAD * (h + 1)])
            row = 2 * HEAD + 3 * h
            levels.append(block[row : row + 1] + block[row + 1 : row + 2] + block[row + 2 : row + 3])
        top = functools.reduce(jnp.maximum, levels)
        shares = [jnp.exp2(level - top) for level in levels]
        total = functools.reduce(jnp.add, shares)
        mixed = functools.reduce(jnp.add, [o * (s / total) for o, s in zip(outs, shares)])
        merged.append(mixed)
    out_ref[:, 0 : 2 * HEAD] = jnp.transpose(jnp.concatenate(merged, axis=0)).astype(jnp.bfloat16)

    r_sent = reduce(
        out_ref, w_ol, w_ow, result_ref, pair_out, pair_in, passed, gone, kept, side_out, side_in, r_send, r_recv
    )

    w_sends = [w_after, w_before, q_onward(True), q_onward(False)]
    w_sends += [q_side(half, way) for half in range(2) for way in (True, False)]
    for step in range(1, 4):
        for half in range(2):
            w_sends += [kv_copy(step, half, True), kv_copy(step, half, False)]
    w_sends += [kv_last(half, way) for half in range(2) for way in (True, False)]
    w_sends += [o_copy(g) for g in range(1, 4)]
    for sent in w_sends + x_sent + r_sent:
        sent.wait_send()


def tables():
    near, freqs = [], []
    for width in (HEAD, ROPE):
        half = width // 2
        freqs.append(10000.0 ** (-np.arange(half) / half))
    freqs = np.concatenate(freqs)
    angles = freqs[:, None] * np.arange(BLK)[None, :]
    near = np.stack([np.cos(angles), np.sin(angles)]).astype(np.float32)
    angles = freqs[:, None] * (BLK * np.arange(128))[None, :]
    far = np.stack([np.cos(angles), np.sin(angles)]).astype(np.float32)
    return near, far


def shards(
    inputs,
    norm_gain,
    latent_query,
    latent_down,
    rope_down,
    latent_gain,
    latent_up,
    window_query,
    window_key,
    window_value,
    sink_logit,
    out_latent,
    out_window,
):
    length_all = BLK * Z * Y
    near, far = tables()
    dma = pltpu.SemaphoreType.DMA
    bf16, f32 = jnp.bfloat16, jnp.float32
    in_vmem = pl.BlockSpec(memory_space=pltpu.VMEM)
    in_smem = pl.BlockSpec(memory_space=pltpu.SMEM)
    in_hbm = pl.BlockSpec(memory_space=pltpu.HBM)
    rows = norm_gain.shape[0]
    return pl.pallas_call(
        functools.partial(layer_kernel, length_all),
        out_shape=pltpu.VMEM((BLK, COLS), bf16),
        in_specs=[in_smem] + [in_hbm] * 14,
        out_specs=in_vmem,
        scratch_shapes=[
            pltpu.VMEM((1, rows), f32),
            pltpu.VMEM((1, latent_gain.shape[0]), f32),
            pltpu.VMEM(near.shape, f32),
            pltpu.VMEM(far.shape, f32),
            pltpu.VMEM((SLIM[3], rows), bf16),
            pltpu.VMEM(latent_down.shape, bf16),
            pltpu.VMEM(window_query.shape, bf16),
            pltpu.VMEM(latent_up.shape, bf16),
            pltpu.VMEM(out_latent.shape, bf16),
            pltpu.VMEM(out_window.shape, bf16),
            pltpu.VMEM((2 * X, BLK, COLS), bf16),
            pltpu.VMEM((BLK, 128), f32),
            pltpu.VMEM((SLIM[3], BLK), f32),
            pltpu.VMEM((BLK, latent_down.shape[1]), f32),
            pltpu.VMEM((BLK, window_query.shape[1]), f32),
            pltpu.VMEM((2 * (NOPE + ROPE), BLK), bf16),
            pltpu.VMEM((BLK, 2 * HEAD), bf16),
            pltpu.VMEM((2 * HEAD, BLK), bf16),
            pltpu.VMEM((BLK, 4 * HEAD), bf16),
            pltpu.VMEM((Z, 2, HALF, 128), bf16),
            pltpu.VMEM((Z, BLK, 128), bf16),
            pltpu.VMEM((Y, 2 * (NOPE + ROPE), BLK), bf16),
            pltpu.VMEM((2 * Y, 256, BLK), bf16),
            pltpu.VMEM((BLK + 2 * WINDOW, 128), bf16),
            *[pltpu.VMEM((BLK, TILE), f32)] * 8,
            pltpu.VMEM((4, 1, BLK), f32),
            pltpu.VMEM((4, 1, BLK), f32),
            pltpu.VMEM((2 * Y, 1, BLK), f32),
            pltpu.VMEM((2 * Y, HEAD + 16, BLK), f32),
            pltpu.VMEM((Y - 1, O_ROWS, BLK), bf16),
            pltpu.VMEM((Y - 1, O_ROWS, BLK), bf16),
            pltpu.VMEM((X, BLK, COLS), bf16),
            pltpu.VMEM((X, BLK, COLS), bf16),
            pltpu.VMEM((2, ROWS, COLS), bf16),
            pltpu.VMEM((2, ROWS, COLS), bf16),
            pltpu.VMEM((4, ROWS, COLS), f32),
            pltpu.VMEM((4, ROWS, COLS), bf16),
            pltpu.VMEM((4, ROWS, COLS), bf16),
            dma((14,)),
            dma((20,)),
            dma((20,)),
            dma((18,)),
            dma((18,)),
            dma((6,)),
            dma((6,)),
            dma((3,)),
            dma((3,)),
            dma((2,)),
            dma((2,)),
            dma((18,)),
            dma((18,)),
        ],
        compiler_params=pltpu.CompilerParams(
            collective_id=1, has_side_effects=True, vmem_limit_bytes=VMEM_LIMIT
        ),
        name="layer",
    )(
        sink_logit,
        inputs,
        norm_gain[None, :],
        latent_gain[None, :],
        near,
        far,
        latent_query.T,
        window_key.T,
        window_value.T,
        rope_down.T,
        latent_down,
        window_query,
        latent_up,
        out_latent,
        out_window,
    )


def solution(mesh):
    in_specs = (
        P("sp", "tp"),
        P(),
        P(None, "tp"),
        P(),
        P(),
        P(),
        P(None, "tp"),
        P(None, "tp"),
        P(None, "tp"),
        P(None, "tp"),
        P("tp"),
        P("tp", None),
        P("tp", None),
    )
    out_specs = P("sp", "tp")
    return jax.shard_map(shards, mesh=mesh, in_specs=in_specs, out_specs=out_specs, check_vma=False)
```
